32 devices in a mesh: ep: 4 (over y, x), tp: 8 (over z, core).
Axes of the slice: x: 2, y: 2, z: 4, core: 2. Of those that a mesh axis runs over, the one named last changes fastest.
Arguments:
- query_rows: bfloat16 [4096, 2048], P('ep', 'tp'), may hold values from -6 to 6
- key_rows: bfloat16 [4096, 2048], P('ep', 'tp'), may hold values from -6 to 6
- value_rows: bfloat16 [4096, 4096], P('ep', 'tp'), may hold values from -6 to 6
- gate_rows: bfloat16 [4096, 4096], P('ep', 'tp'), may hold values from -6 to 6
- log_decay: float32 [16, 4096], P('tp', 'ep'), may hold values from -1.5 to 0
- out_weight: bfloat16 [4096, 2048], P('tp'), may hold values from -0.09375 to 0.09375
- channel_input: bfloat16 [1536, 2048], P(('ep', 'tp')), may hold values from -6 to 6
- norm_gain: float32 [2048], replicated, may hold values from 0.1 to 1.9
- routes: int32 [1536, 2], P(('ep', 'tp')), may hold values from 0 to 7, all different within a row; in each aligned block of 48 rows (0 to 47, 48 to 95, ...) at most 16 rows name the same one
- route_weight: float32 [1536, 2], P(('ep', 'tp')), may hold values from 0.2 to 1.5
- expert_gate: bfloat16 [8, 2048, 2048], P('ep', None, 'tp'), may hold values from -0.125 to 0.125
- expert_up: bfloat16 [8, 2048, 2048], P('ep', None, 'tp'), may hold values from -0.125 to 0.125
- expert_down: bfloat16 [8, 2048, 2048], P('ep', 'tp'), may hold values from -0.125 to 0.125
- shared_gate: bfloat16 [2048, 2048], P(None, 'tp'), may hold values from -0.125 to 0.125
- shared_up: bfloat16 [2048, 2048], P(None, 'tp'), may hold values from -0.125 to 0.125
- shared_down: bfloat16 [2048, 2048], P('tp'), may hold values from -0.125 to 0.125
Outputs:
- mixer_out: bfloat16 [4096, 2048], P(('ep', 'tp'))
- channel_out: bfloat16 [1536, 2048], P(('ep', 'tp'))
The draws below stay inside these ranges and needn't reach their ends.
Inputs may be any that keep to these rules, and one draw needn't show every extreme that they name: `routes`: each row names 2 different experts; among the rows of one device no expert is named more than 16 times, a bound that some block reaches.
All inputs are finite; a program needn't handle non-finite values.
Results may differ from the reference program's by a relative error of at most 0.02.
Values may be sent and summed in bfloat16 or wider, within the bound.
A program may use at most 128 MiB of HBM per device.

```python
import math
import jax
import jax.numpy as jnp
import numpy as np
from jax import lax

D = 2048
RETENTION_HEADS = 16
DK = 128
DV = 256
BLOCK = 128
TOK_A = 1024
FF = 2048
TOPK = 2
T_M = 48
SEQUENCE_LENGTH = 4096
QK_WIDTH = 2048
V_WIDTH = 4096
EXPERTS = 8
TOKENS_M = 1536
CAP = 16
N_EP = 4
N_TP = 8


def draw_log_decay(key, part):
    key_pieces_list = jax.random.split(jax.random.fold_in(key, 11), 7)
    slow_share = 0.5
    slow_heads = jax.random.uniform(key_pieces_list[0], (RETENTION_HEADS,)) < slow_share
    whole_loss = jax.random.uniform(key_pieces_list[1], (RETENTION_HEADS,), minval=0.1, maxval=0.5)
    fast_rate = jax.random.uniform(key_pieces_list[2], (RETENTION_HEADS,), minval=1.0 / 100.0, maxval=1.0 / 30.0)
    decay_rate = jnp.where(slow_heads, whole_loss / SEQUENCE_LENGTH, fast_rate)
    span_count = SEQUENCE_LENGTH // TOK_A
    block_factor = jnp.exp(jax.random.uniform(key_pieces_list[3], (RETENTION_HEADS, span_count), minval=-0.7, maxval=0.7))
    block_factor = jnp.repeat(block_factor, TOK_A, axis=1)
    jitter = jax.random.uniform(key_pieces_list[4], (RETENTION_HEADS, SEQUENCE_LENGTH), minval=0.5, maxval=1.5)
    steady_level = -(decay_rate[:, None] * block_factor * jitter)
    surge_position = jax.random.randint(key_pieces_list[5], (RETENTION_HEADS, 2), 0, SEQUENCE_LENGTH)
    surge_extent = jnp.log(jax.random.uniform(key_pieces_list[6], (RETENTION_HEADS, 2), minval=0.5, maxval=0.8))
    head_number = jnp.broadcast_to(jnp.arange(RETENTION_HEADS)[:, None], (RETENTION_HEADS, 2))
    surge_list = jnp.zeros((RETENTION_HEADS, SEQUENCE_LENGTH), jnp.float32).at[head_number, surge_position].add(surge_extent)
    return (steady_level + surge_list).astype(jnp.float32)


def block_scale(own_key, shape, cuts, least, largest):
    loudness = 1.0
    for dim, shards_of in cuts:
        steps = jax.random.uniform(jax.random.fold_in(jax.random.fold_in(own_key, 6), dim), (shards_of,), jnp.float32, least / len(cuts), largest / len(cuts))
        loudness = loudness * jnp.repeat(jnp.exp(steps), shape[dim] // shards_of).reshape((-1,) + (1,) * (len(shape) - 1 - dim))
    return loudness


def shared_out(rng, own, number, rows, number_of, top, most, slope):
    sequence = jax.random.permutation(rng, number_of)
    crowded, usual = shares(number_of, rows * top, most, slope, True), shares(number_of, rows * top, most, slope, False)
    places = jnp.arange(number_of)

    def named(tallies, rotation):
        used = int((tallies > 0).sum())
        fixed = max(1, used // 4)
        passed = fixed + (places - fixed + rotation * (used - fixed)) % max(1, number_of - fixed)
        return jnp.zeros((number_of,), jnp.int32).at[sequence[jnp.where(places < fixed, places, passed)]].set(jnp.asarray(tallies, jnp.int32))

    tallies = jnp.where(number % 4 == 0, named(crowded, number // 4), named(usual, number - number // 4 - 1))
    mixed = jax.random.permutation(jax.random.fold_in(own, 3), number_of)
    giver, sink = mixed[0:number_of // 2 * 2:2], mixed[1:number_of // 2 * 2:2]
    slack = jnp.minimum(tallies[giver] - 1, most - tallies[sink]) // 2
    slack = jnp.where((giver == sequence[0]) | (sink == sequence[0]) | (tallies[sink] == 0), 0, jnp.maximum(slack, 0))
    passed = jax.random.randint(jax.random.fold_in(own, 4), (number_of // 2,), 0, 1 << 20) % (slack + 1)
    tallies = tallies.at[giver].add(-passed).at[sink].add(passed)
    members = jnp.searchsorted(jnp.cumsum(tallies), jnp.arange(rows * top), side="right").astype(jnp.int32)
    listing = members.reshape(top, rows).T
    listing = listing[jax.random.permutation(jax.random.fold_in(own, 1), rows)]
    rotation = jax.random.randint(jax.random.fold_in(own, 2), (rows, 1), 0, top)
    return jnp.take_along_axis(listing, (jnp.arange(top)[None, :] + rotation) % top, axis=1)


def shares(amount, total, most, slope, full):
    loads = [(1 << 20) // math.isqrt(standing ** slope) + 1 for standing in range(1, amount + 1)]
    largest = most if full else min(most, max(-(-total // amount), total * loads[0] // sum(loads)))
    least = 1 if total - largest >= amount - 1 else 0
    given, spare = [largest] + [least] * (amount - 1), total - largest - least * (amount - 1)
    while spare > 0:
        free = [i for i in range(1, amount) if given[i] < largest] or [i for i in range(1, amount) if given[i] < most]
        whole, left = sum([loads[i] for i in free]), spare
        for i in free:
            addition = min(most - given[i], max(1, left * loads[i] // whole), spare)
            given[i] = given[i] + addition
            spare = spare - addition
    return np.array(given)


def noise(key, shape, scale, most, pieces=(), kind=jnp.bfloat16):
    values = scale * jax.random.normal(key, shape, jnp.float32)
    if pieces:
        values = values * block_scale(key, shape, pieces, -0.22, 0.18)
    return jnp.clip(values, -most, most).astype(kind)


def setup_inputs(seed: int = 0) -> dict:
    arg_keys = jax.random.split(jax.random.key(seed), 17)
    query_rows = noise(arg_keys[0], (SEQUENCE_LENGTH, QK_WIDTH), 1.0, 6.0, ((0, 4), (1, 8)))
    key_rows = noise(arg_keys[1], (SEQUENCE_LENGTH, QK_WIDTH), 1.0, 6.0, ((0, 4), (1, 8)))
    value_rows = noise(arg_keys[2], (SEQUENCE_LENGTH, V_WIDTH), 1.0, 6.0, ((0, 4), (1, 8)))
    gate_rows = noise(arg_keys[3], (SEQUENCE_LENGTH, V_WIDTH), 1.0, 6.0, ((0, 4), (1, 8)))
    log_decay = draw_log_decay(jax.random.fold_in(arg_keys[16], 71), 0)
    out_weight = noise(arg_keys[5], (V_WIDTH, D), V_WIDTH ** -0.5, 0.09375, ((0, 8),))
    channel_input = noise(arg_keys[6], (TOKENS_M, D), 1.0, 6.0, ((0, 32),))
    norm_gain = jnp.clip(1.0 + 0.18 * jax.random.normal(arg_keys[7], (D,), jnp.float32), 0.1, 1.9)
    routes_keys = jax.random.split(jax.random.fold_in(arg_keys[8], 1), TOKENS_M // T_M)
    routes_turns = jax.random.permutation(jax.random.fold_in(arg_keys[8], 3), TOKENS_M // T_M)
    routes = jax.vmap(lambda own, number: shared_out(jax.random.fold_in(arg_keys[8], 2), own, number, T_M, EXPERTS, TOPK, CAP, 1))(routes_keys, routes_turns).reshape((TOKENS_M, TOPK))
    route_weight = jnp.clip(0.2 + 1.3 * jax.random.uniform(arg_keys[9], (TOKENS_M, TOPK), jnp.float32) ** block_scale(arg_keys[9], (TOKENS_M, TOPK), ((0, 32),), -0.2, 0.2), 0.2, 1.5)
    expert_gate = noise(arg_keys[10], (EXPERTS, D, FF), D ** -0.5, 0.125, ((0, 4), (2, 8)))
    expert_up = noise(arg_keys[11], (EXPERTS, D, FF), D ** -0.5, 0.125, ((0, 4), (2, 8)))
    expert_down = noise(arg_keys[12], (EXPERTS, FF, D), FF ** -0.5, 0.125, ((0, 4), (1, 8)))
    shared_gate = noise(arg_keys[13], (D, FF), D ** -0.5, 0.125, ((1, 8),))
    shared_up = noise(arg_keys[14], (D, FF), D ** -0.5, 0.125, ((1, 8),))
    shared_down = noise(arg_keys[15], (FF, D), FF ** -0.5, 0.125, ((0, 8),))
    return {"query_rows": query_rows, "key_rows": key_rows, "value_rows": value_rows, "gate_rows": gate_rows, "log_decay": log_decay, "out_weight": out_weight, "channel_input": channel_input, "norm_gain": norm_gain, "routes": routes, "route_weight": route_weight, "expert_gate": expert_gate, "expert_up": expert_up, "expert_down": expert_down, "shared_gate": shared_gate, "shared_up": shared_up, "shared_down": shared_down}


epsilon = 1e-06
turn_base = 10000.0

def turn_heads(rows, position):
    half_width = rows.shape[-1] // 2
    inverse = turn_base ** (-jnp.arange(half_width, dtype=jnp.float32) / half_width)
    angles = position[:, None] * inverse[None, :]
    cosine = jnp.cos(angles)[:, None, :]
    sine = jnp.sin(angles)[:, None, :]
    widened = rows.astype(jnp.float32)
    first_half = widened[..., :half_width]
    second_half = widened[..., half_width:]
    turned = jnp.concatenate([first_half * cosine - second_half * sine, second_half * cosine + first_half * sine], axis=-1)
    return turned.astype(jnp.bfloat16)

def blocked_product(left, right, parts):
    width = right.shape[0] // parts

    def add_block(index, total):
        columns = lax.dynamic_slice_in_dim(left, index * width, width, 1)
        block_rows = lax.dynamic_slice_in_dim(right, index * width, width, 0)
        partial_sum = jnp.dot(columns, block_rows, preferred_element_type=jnp.float32).astype(jnp.bfloat16)
        partial_sum = lax.optimization_barrier(partial_sum)
        return total + partial_sum.astype(jnp.float32)
    return lax.fori_loop(0, parts, add_block, jnp.zeros((left.shape[0], right.shape[1]), jnp.float32))

def swiglu_hidden(rows, gate_weight, up_weight):
    gate_part = jnp.dot(rows, gate_weight, preferred_element_type=jnp.float32)
    up_part = jnp.dot(rows, up_weight, preferred_element_type=jnp.float32)
    return (jax.nn.silu(gate_part) * up_part).astype(jnp.bfloat16)

def retention(queries, keys_turned, values, log_decay):
    block_count = SEQUENCE_LENGTH // BLOCK
    query_blocks = queries.reshape(block_count, BLOCK, RETENTION_HEADS, DK)
    key_blocks = keys_turned.reshape(block_count, BLOCK, RETENTION_HEADS, DK)
    value_blocks = values.reshape(block_count, BLOCK, RETENTION_HEADS, DV)
    decay_blocks = jnp.transpose(log_decay.reshape(RETENTION_HEADS, block_count, BLOCK), (1, 0, 2))
    lower = jnp.arange(BLOCK)[:, None] >= jnp.arange(BLOCK)[None, :]
    highest = lax.Precision.HIGHEST

    def advance(state, inputs):
        query_block, key_block, value_block, decay_block = inputs
        running = jnp.cumsum(decay_block, axis=1)
        query_wide = query_block.astype(jnp.float32)
        key_wide = key_block.astype(jnp.float32)
        value_wide = value_block.astype(jnp.float32)
        scores = jnp.einsum('ihk,jhk->hij', query_wide, key_wide, precision=highest)
        spread = running[:, :, None] - running[:, None, :]
        weights = jnp.where(lower, scores * jnp.exp(jnp.where(lower, spread, 0.0)), 0.0).astype(jnp.bfloat16)
        intra = jnp.einsum('hij,jhe->ihe', weights.astype(jnp.float32), value_wide, precision=highest)
        query_decayed = query_wide * jnp.exp(running).T[:, :, None]
        inter = jnp.einsum('ihk,hke->ihe', query_decayed, state, precision=highest)
        block_end = running[:, -1]
        key_decayed = key_wide * jnp.exp(block_end[:, None] - running).T[:, :, None]
        update = jnp.einsum('jhk,jhe->hke', key_decayed, value_wide, precision=highest)
        new_state = jnp.exp(block_end)[:, None, None] * state + update
        return (new_state, intra + inter)
    start_state = jnp.zeros((RETENTION_HEADS, DK, DV), jnp.float32)
    _, outputs = lax.scan(advance, start_state, (query_blocks, key_blocks, value_blocks, decay_blocks))
    return outputs.reshape(SEQUENCE_LENGTH, RETENTION_HEADS, DV)

def reference(query_rows, key_rows, value_rows, gate_rows, log_decay, out_weight, channel_input, norm_gain, routes, route_weight, expert_gate, expert_up, expert_down, shared_gate, shared_up, shared_down):
    position = jnp.arange(SEQUENCE_LENGTH, dtype=jnp.int32).astype(jnp.float32)
    queries = turn_heads(query_rows.reshape(SEQUENCE_LENGTH, RETENTION_HEADS, DK), position)
    keys_turned = turn_heads(key_rows.reshape(SEQUENCE_LENGTH, RETENTION_HEADS, DK), position)
    retained = retention(queries, keys_turned, value_rows.reshape(SEQUENCE_LENGTH, RETENTION_HEADS, DV), log_decay)
    scaled = retained * lax.rsqrt(lax.optimization_barrier(jnp.mean(retained * retained, axis=-1, keepdims=True)) + epsilon)
    gate_wide = gate_rows.astype(jnp.float32).reshape(SEQUENCE_LENGTH, RETENTION_HEADS, DV)
    gated = (jax.nn.silu(gate_wide) * scaled).astype(jnp.bfloat16).reshape(SEQUENCE_LENGTH, RETENTION_HEADS * DV)
    mixer_out = blocked_product(gated, out_weight, N_TP).astype(jnp.bfloat16)
    widened = channel_input.astype(jnp.float32)
    normed = (widened * lax.rsqrt(lax.optimization_barrier(jnp.mean(widened * widened, axis=-1, keepdims=True)) + epsilon) * norm_gain).astype(jnp.bfloat16)
    shared_result = blocked_product(swiglu_hidden(normed, shared_gate, shared_up), shared_down, N_TP)
    flat_expert = routes.reshape(-1)
    assign_count = flat_expert.shape[0]
    flat_token = jnp.arange(assign_count, dtype=jnp.int32) // TOPK
    flat_weight = route_weight.reshape(-1)
    limit = N_EP * N_TP * CAP

    def add_expert(total, expert):
        chosen = jnp.nonzero(flat_expert == expert, size=limit, fill_value=assign_count)[0].astype(jnp.int32)
        valid = chosen < assign_count
        safe = jnp.minimum(chosen, assign_count - 1)
        token_index = flat_token[safe]
        weight = jnp.where(valid, flat_weight[safe], 0.0)
        hidden = swiglu_hidden(normed[token_index], expert_gate[expert], expert_up[expert])
        result = blocked_product(hidden, expert_down[expert], N_TP).astype(jnp.bfloat16)
        result = lax.optimization_barrier(result)
        return (total.at[token_index].add(weight[:, None] * result.astype(jnp.float32)), None)
    routed, _ = lax.scan(add_expert, jnp.zeros((TOKENS_M, D), jnp.float32), jnp.arange(EXPERTS, dtype=jnp.int32))
    channel_out = (shared_result + routed).astype(jnp.bfloat16)
    return (mixer_out, channel_out)
```

```python
import functools
import math

import jax
import jax.numpy as jnp
import numpy as np
from jax import lax
from jax.experimental import pallas as pl
from jax.experimental.pallas import tpu as pltpu
from jax.sharding import PartitionSpec as P

BLOCK = 128
CORES = 2
KERNEL_VMEM = 67043328

epsilon = 1e-06
turn_base = 10000.0


def shift_chips(array, r, count):
    pairs = [
        (z * CORES + c, (z + r) % count * CORES + c) for z in range(count) for c in range(CORES)
    ]
    return lax.ppermute(array, "tp", pairs)


def line_gather(array, count):
    return jnp.stack([array] + [shift_chips(array, r, count) for r in range(1, count)])


def line_scatter(part, count):
    total = part(0).astype(jnp.float32)
    for r in range(1, count):
        total = total + shift_chips(part(r), r, count).astype(jnp.float32)
    return total


def swap_cores(array, tp_count):
    return lax.ppermute(array, "tp", [(i, i ^ 1) for i in range(tp_count)])


def swap_ep(array, k, ep_count):
    return lax.ppermute(array, "ep", [(i, i ^ k) for i in range(ep_count)])


def turned(rows, cosine, sine):
    wide = rows.astype(jnp.float32)
    return (wide * cosine + pltpu.roll(wide, wide.shape[1] // 2, 1) * sine).astype(jnp.bfloat16)


def state_kernel(key_ref, value_ref, cosine_ref, sine_ref, fade_ref, state_ref):
    heads, key_width, value_width = state_ref.shape
    for h in range(heads):
        keys = turned(
            key_ref[:, h * key_width : (h + 1) * key_width], cosine_ref[...], sine_ref[...]
        )
        faded = (keys.astype(jnp.float32) * fade_ref[:, h : h + 1]).astype(jnp.bfloat16)
        state_ref[h] = lax.dot_general(
            faded,
            value_ref[:, h * value_width : (h + 1) * value_width],
            (((0,), (0,)), ((), ())),
            preferred_element_type=jnp.float32,
        ).astype(state_ref.dtype)


def retention_kernel(
    query_ref, key_ref, value_ref, gate_ref, cosine_ref, sine_ref, column_ref, row_ref,
    entry_ref, out_ref, state,
):
    heads, key_width, value_width = state.shape

    @pl.when(pl.program_id(0) == 0)
    def _():
        state[...] = entry_ref[...]

    cosine, sine = cosine_ref[...], sine_ref[...]
    lower = lax.broadcasted_iota(jnp.int32, (BLOCK, BLOCK), 0) >= lax.broadcasted_iota(
        jnp.int32, (BLOCK, BLOCK), 1
    )
    for h in range(heads):
        key_cut = slice(h * key_width, (h + 1) * key_width)
        value_cut = slice(h * value_width, (h + 1) * value_width)
        queries = turned(query_ref[:, key_cut], cosine, sine)
        keys = turned(key_ref[:, key_cut], cosine, sine)
        values = value_ref[:, value_cut]
        column = column_ref[:, h : h + 1]
        row = row_ref[0, h : h + 1, :]
        end = column_ref[BLOCK - 1 : BLOCK, h : h + 1]
        scores = lax.dot_general(
            queries, keys, (((1,), (1,)), ((), ())), preferred_element_type=jnp.float32
        )
        spread = jnp.exp(jnp.where(lower, column - row, 0.0))
        weights = jnp.where(lower, scores * spread, 0.0).astype(jnp.bfloat16)
        before = state[h]
        retained = jnp.dot(weights, values, preferred_element_type=jnp.float32)
        retained = retained + jnp.exp(column) * jnp.dot(
            queries, before.astype(jnp.bfloat16), preferred_element_type=jnp.float32
        )
        faded = (keys.astype(jnp.float32) * jnp.exp(end - column)).astype(jnp.bfloat16)
        state[h] = jnp.exp(end) * before + lax.dot_general(
            faded, values, (((0,), (0,)), ((), ())), preferred_element_type=jnp.float32
        )
        scale = lax.rsqrt(jnp.mean(retained * retained, axis=1, keepdims=True) + epsilon)
        gate = gate_ref[:, value_cut].astype(jnp.float32)
        out_ref[:, value_cut] = (gate / (1.0 + jnp.exp(-gate)) * (retained * scale)).astype(
            jnp.bfloat16
        )


def retention(query_rows, key_rows, value_rows, gate_rows, log_decay):
    tokens = query_rows.shape[0]
    heads = log_decay.shape[0]
    key_width = query_rows.shape[1] // heads
    value_width = value_rows.shape[1] // heads
    blocks = tokens // BLOCK
    ep_count, ep_index = lax.axis_size("ep"), lax.axis_index("ep")
    half = key_width // 2
    position = (ep_index * tokens + jnp.arange(tokens, dtype=jnp.int32)).astype(jnp.float32)
    inverse = turn_base ** (-jnp.arange(half, dtype=jnp.float32) / half)
    angles = position[:, None] * inverse[None, :]
    cosine, sine = jnp.cos(angles), jnp.sin(angles)
    cosine = jnp.concatenate([cosine, cosine], axis=1)
    sine = jnp.concatenate([-sine, sine], axis=1)
    running = jnp.cumsum(log_decay.reshape(heads, blocks, BLOCK), axis=2)
    ends = running[:, :, -1]
    later = jnp.sum(ends, axis=1, keepdims=True) - jnp.cumsum(ends, axis=1)
    later = jnp.minimum(later, 0.0)
    fade = jnp.exp(ends[:, :, None] - running + later[:, :, None]).reshape(heads, tokens).T
    total = jnp.sum(ends, axis=1)
    vmem = pl.BlockSpec(memory_space=pltpu.VMEM)
    own_state = pl.pallas_call(
        state_kernel,
        out_shape=jax.ShapeDtypeStruct((heads, key_width, value_width), jnp.bfloat16),
        in_specs=[vmem] * 5,
        out_specs=vmem,
        cost_estimate=pl.CostEstimate(
            flops=2 * tokens * heads * key_width * value_width * 4,
            bytes_accessed=8 << 20,
            transcendentals=0,
        ),
    )(key_rows, value_rows, cosine, sine, fade)
    totals_sent = jnp.broadcast_to(total[:, None], (heads, 128))
    states, totals = [], [total]
    for k in range(1, ep_count):
        states.append(swap_ep(own_state, k, ep_count))
        totals.append(swap_ep(totals_sent, k, ep_count)[:, 0])
    entry = jnp.zeros((heads, key_width, value_width), jnp.float32)
    for k in range(1, ep_count):
        source = ep_index ^ k
        passed = jnp.zeros_like(total)
        for m in range(1, ep_count):
            between = ((ep_index ^ m) > source) & ((ep_index ^ m) < ep_index)
            passed = passed + jnp.where(between, totals[m], 0.0)
        share = jnp.where(source < ep_index, jnp.exp(passed), 0.0)
        entry = entry + share[:, None, None] * states[k - 1].astype(jnp.float32)
    columns = running.reshape(heads, tokens).T
    rows = running.transpose(1, 0, 2)
    by_block = lambda width: pl.BlockSpec((BLOCK, width), lambda n: (n, 0))
    whole = pl.BlockSpec((heads, key_width, value_width), lambda n: (0, 0, 0))
    return pl.pallas_call(
        retention_kernel,
        out_shape=jax.ShapeDtypeStruct((tokens, heads * value_width), jnp.bfloat16),
        grid=(blocks,),
        in_specs=[
            by_block(heads * key_width),
            by_block(heads * key_width),
            by_block(heads * value_width),
            by_block(heads * value_width),
            by_block(key_width),
            by_block(key_width),
            by_block(heads),
            pl.BlockSpec((1, heads, BLOCK), lambda n: (n, 0, 0)),
            whole,
        ],
        out_specs=by_block(heads * value_width),
        scratch_shapes=[pltpu.VMEM((heads, key_width, value_width), jnp.float32)],
        cost_estimate=pl.CostEstimate(
            flops=8 << 30, bytes_accessed=24 << 20, transcendentals=0
        ),
    )(query_rows, key_rows, value_rows, gate_rows, cosine, sine, columns, rows, entry)


def gated_pair(gate_part, up_part):
    return (jax.nn.silu(gate_part) * up_part).astype(jnp.bfloat16)


def summed(a, b):
    return (a.astype(jnp.float32) + b.astype(jnp.float32)).astype(jnp.bfloat16)


def flip(index, k):
    turned_index, bit = index, 1
    while bit <= k:
        if k & bit:
            turned_index = turned_index + bit - 2 * bit * ((index // bit) % 2)
        bit *= 2
    return turned_index


def line_order(chips):
    orders = []
    for z in range(chips):
        right, left = list(range(chips - 1, z, -1)), list(range(z))
        order = []
        while right or left:
            if len(right) >= len(left) and right:
                order.append(right.pop(0))
            elif left:
                order.append(left.pop(0))
        orders.append(order + [z])
    return orders


def pick(table, index):
    chosen = 0
    for i, entry in enumerate(table):
        chosen = chosen + jnp.where(index == i, entry, 0)
    return chosen


def whole_kernel(
    sizes,
    channel_ref, gain_ref, routes_ref, weight_ref, decay_ref, near_ref, far_ref,
    query_any, key_any, value_any, gate_any, out_any, eg_any, eu_any, ed_any, sg_any, su_any,
    sd_any,
    mixer_ref, channel_out_ref,
    query, key, value, gate, out_w, eg, eu, ed, sg, su, sd,
    gathered, notes, slots, arrived, result_twin, result_in, result, returned,
    shared_twin, shared_in, shared_own, channel, channel_right, channel_left,
    mix_twin, mix_in, mix_own, mix_right, mix_left,
    gated, keys_turned, before, entry, state_send, state_in, total_send, total_in, prefix,
    decay_flat, run_row, run_col, state,
    local_sem, g_send, g_recv, n_send, n_recv, tg_send, tg_recv, d_send, d_recv, ta_send, ta_recv,
    ty_send, ty_recv, th_send, th_recv, r_send, r_recv, s_send, s_recv, o_send, o_recv,
    tp_send, tp_recv, m_send, m_right, m_left, c_send, c_right, c_left,
):
    ep_count, chips, capacity = sizes
    f32, bf16 = jnp.float32, jnp.bfloat16
    tokens_here, width = channel_ref.shape
    topk = routes_ref.shape[1]
    local_experts = eg.shape[0]
    block_rows = local_experts * capacity
    slot_count = ep_count * block_rows
    heads, key_width, value_width = state.shape
    blocks = before.shape[0]
    mixer_count = mixer_ref.shape[0]
    ep_index, tp_index = lax.axis_index("ep"), lax.axis_index("tp")
    chip, core = tp_index // CORES, tp_index % CORES
    twin = tp_index + 1 - 2 * core
    orders = line_order(chips)
    order = [pick([row[i] for row in orders], chip) for i in range(chips - 1)] + [chip]

    def to_tp(src, dst, send, recv, target):
        return pltpu.make_async_remote_copy(
            src_ref=src, dst_ref=dst, send_sem=send, recv_sem=recv,
            device_id={"tp": target}, device_id_type=pl.DeviceIdType.MESH,
        )

    def to_ep(src, dst, send, recv, target):
        return pltpu.make_async_remote_copy(
            src_ref=src, dst_ref=dst, send_sem=send, recv_sem=recv,
            device_id={"ep": target}, device_id_type=pl.DeviceIdType.MESH,
        )

    barrier = pltpu.get_barrier_semaphore()
    for r in range(1, chips):
        pl.semaphore_signal(
            barrier, inc=1, device_id={"tp": (chip + r) % chips * CORES + core},
            device_id_type=pl.DeviceIdType.MESH,
        )
    pl.semaphore_signal(
        barrier, inc=1, device_id={"tp": twin}, device_id_type=pl.DeviceIdType.MESH
    )
    for k in range(1, ep_count):
        pl.semaphore_signal(
            barrier, inc=1, device_id={"ep": flip(ep_index, k)},
            device_id_type=pl.DeviceIdType.MESH,
        )

    pairs = [
        (key_any, key), (value_any, value), (query_any, query), (gate_any, gate),
        (out_any, out_w), (sg_any, sg), (su_any, su), (sd_any, sd), (eg_any, eg), (eu_any, eu),
        (ed_any, ed),
    ]
    loads = [pltpu.make_async_copy(s, d, local_sem.at[i]) for i, (s, d) in enumerate(pairs)]
    for load in loads:
        load.start()

    wide = channel_ref[...].astype(f32)
    normed = (
        wide * lax.rsqrt(jnp.mean(wide * wide, axis=-1, keepdims=True) + epsilon) * gain_ref[...]
    ).astype(bf16)
    gathered[chip, 0] = normed
    lane = lax.broadcasted_iota(jnp.int32, (tokens_here, 128), 1)
    routed_to = [routes_ref[:, t : t + 1] for t in range(topk)]
    named = [(route == lane).astype(f32) for route in routed_to]
    earlier = (
        lax.broadcasted_iota(jnp.int32, (tokens_here, tokens_here), 0)
        > lax.broadcasted_iota(jnp.int32, (tokens_here, tokens_here), 1)
    ).astype(bf16)
    ahead = jnp.dot(earlier, sum(named).astype(bf16), preferred_element_type=f32)
    noted = jnp.zeros((tokens_here, 128), f32)
    for t in range(topk):
        rank = jnp.sum(ahead * named[t], axis=1, keepdims=True)
        slot = routed_to[t].astype(f32) * capacity + rank
        noted = jnp.where(lane == t, slot, noted)
        noted = jnp.where(lane == topk + t, weight_ref[:, t : t + 1], noted)
    notes[chip] = noted

    pl.semaphore_wait(barrier, chips + ep_count - 1)

    def gather_row(q, target):
        return to_tp(
            gathered.at[q, 0], gathered.at[q, 0], g_send.at[target], g_recv.at[q],
            target * CORES + core,
        )

    def gather_note(q, target):
        return to_tp(
            notes.at[q], notes.at[q], n_send.at[target], n_recv.at[q], target * CORES + core
        )

    def twin_row(q):
        return to_tp(
            gathered.at[q, 0], gathered.at[q, 1], tg_send.at[q], tg_recv.at[q], twin
        )

    near_first = order[:-1][::-1]
    for target in near_first:
        gather_row(chip, target).start()
        gather_note(chip, target).start()
    twin_row(chip).start()

    slot_lane = lax.broadcasted_iota(jnp.int32, (tokens_here, slot_count), 1).astype(f32)

    def dispatch_copy(q, k):
        target = flip(ep_index, k)
        return to_ep(
            slots.at[q, target], arrived.at[q, 0, ep_index], d_send.at[q, k], d_recv.at[q, k],
            target,
        )

    def dispatch(q):
        placing = sum(
            (notes[q][:, t : t + 1] == slot_lane).astype(f32) for t in range(topk)
        ).astype(bf16)
        rows = lax.dot_general(
            placing, gathered[q, 0], (((0,), (0,)), ((), ())), preferred_element_type=f32
        ).astype(bf16)
        slots[q] = rows.reshape(ep_count, block_rows, width)
        for k in range(1, ep_count):
            dispatch_copy(q, k).start()
        arrived[q, 0, ep_index] = slots[q, ep_index]

    def take_row(q):
        gather_row(q, q).wait_recv()
        gather_note(q, q).wait_recv()
        twin_row(q).start()
        dispatch(q)

    dispatch(chip)

    for n in range(blocks):
        decay_flat[n * heads : (n + 1) * heads, :] = decay_ref[:, n * BLOCK : (n + 1) * BLOCK]
    upper = (
        lax.broadcasted_iota(jnp.int32, (BLOCK, BLOCK), 0)
        <= lax.broadcasted_iota(jnp.int32, (BLOCK, BLOCK), 1)
    )
    lower = (
        lax.broadcasted_iota(jnp.int32, (BLOCK, BLOCK), 0)
        >= lax.broadcasted_iota(jnp.int32, (BLOCK, BLOCK), 1)
    )
    flat = decay_flat[...]
    by_row = jnp.dot(
        flat, upper.astype(f32), preferred_element_type=f32, precision=lax.Precision.HIGHEST
    )
    by_col = lax.dot_general(
        lower.astype(f32), flat, (((1,), (1,)), ((), ())), preferred_element_type=f32,
        precision=lax.Precision.HIGHEST,
    )
    for n in range(blocks):
        run_row[n, 0:heads, :] = by_row[n * heads : (n + 1) * heads, :]
        run_col[n, :, 0:heads] = by_col[:, n * heads : (n + 1) * heads]

    def turns(n):
        far = far_ref[ep_index * blocks + n]
        far_cos, far_sin = far[0:1, :], far[1:2, :]
        near_cos, near_sin = near_ref[0], near_ref[1]
        return near_cos * far_cos - near_sin * far_sin, near_sin * far_cos + near_cos * far_sin

    loads[0].wait()
    loads[1].wait()
    state[...] = jnp.zeros_like(state)
    total_send[...] = jnp.zeros_like(total_send)

    def first_pass(n, carry):
        at = pl.ds(pl.multiple_of(n * BLOCK, BLOCK), BLOCK)
        cosine, sine = turns(n)
        prefix[n] = total_send[...]
        for h in range(heads):
            key_cut = slice(h * key_width, (h + 1) * key_width)
            value_cut = slice(h * value_width, (h + 1) * value_width)
            keys = turned(key[at, key_cut], cosine, sine)
            keys_turned[at, key_cut] = keys
            column = run_col[n, :, h : h + 1]
            end = run_row[n, h : h + 1, BLOCK - 1 : BLOCK]
            faded = (keys.astype(f32) * jnp.exp(end - column)).astype(bf16)
            held = state[h]
            before[n, h] = held
            state[h] = jnp.exp(end) * held + lax.dot_general(
                faded, value[at, value_cut], (((0,), (0,)), ((), ())),
                preferred_element_type=f32,
            )
            total_send[h : h + 1, :] = total_send[h : h + 1, :] + end
        return carry

    lax.fori_loop(0, blocks, first_pass, 0)
    state_send[...] = state[...].astype(bf16)

    def state_copy(k):
        return to_ep(
            state_send, state_in.at[k], s_send.at[k], s_recv.at[k], flip(ep_index, k)
        )

    def total_copy(k):
        return to_ep(
            total_send, total_in.at[k], o_send.at[k], o_recv.at[k], flip(ep_index, k)
        )

    for k in range(1, ep_count):
        state_copy(k).start()
        total_copy(k).start()

    take_row(near_first[0])

    for k in range(1, ep_count):
        state_copy(k).wait_recv()
        total_copy(k).wait_recv()
    for k in range(1, ep_count):
        source = flip(ep_index, k)
        passed = jnp.zeros(total_send.shape, f32)
        for m in range(1, ep_count):
            between = (flip(ep_index, m) > source) & (flip(ep_index, m) < ep_index)
            passed = passed + jnp.where(between, total_in[m], 0.0)
        share = jnp.where(source < ep_index, jnp.exp(passed), 0.0)
        for h in range(heads):
            term = share[h : h + 1, 0:1] * state_in[k, h].astype(f32)
            entry[h] = term if k == 1 else entry[h] + term

    loads[2].wait()
    loads[3].wait()

    def second_pass(n, carry):
        at = pl.ds(pl.multiple_of(n * BLOCK, BLOCK), BLOCK)
        cosine, sine = turns(n)
        for h in range(heads):
            key_cut = slice(h * key_width, (h + 1) * key_width)
            value_cut = slice(h * value_width, (h + 1) * value_width)
            queries = turned(query[at, key_cut], cosine, sine)
            keys = keys_turned[at, key_cut]
            values = value[at, value_cut]
            column = run_col[n, :, h : h + 1]
            row = run_row[n, h : h + 1, :]
            scores = lax.dot_general(
                queries, keys, (((1,), (1,)), ((), ())), preferred_element_type=f32
            )
            spread = jnp.exp(jnp.where(lower, column - row, 0.0))
            weights = jnp.where(lower, scores * spread, 0.0).astype(bf16)
            held = before[n, h] + jnp.exp(prefix[n, h : h + 1, 0:1]) * entry[h]
            retained = jnp.dot(weights, values, preferred_element_type=f32)
            retained = retained + jnp.exp(column) * jnp.dot(
                queries, held.astype(bf16), preferred_element_type=f32
            )
            scale = lax.rsqrt(jnp.mean(retained * retained, axis=1, keepdims=True) + epsilon)
            gates = gate[at, value_cut].astype(f32)
            gated[at, value_cut] = (
                gates / (1.0 + jnp.exp(-gates)) * (retained * scale)
            ).astype(bf16)
        return carry

    lax.fori_loop(0, blocks, second_pass, 0)

    loads[4].wait()

    def twin_mix(d):
        return to_tp(mix_twin.at[d], mix_in.at[d], tp_send.at[d], tp_recv.at[d], twin)

    def project(d, which, into):
        start = pl.multiple_of((d * CORES + which) * mixer_count, mixer_count)
        into[d] = jnp.dot(
            gated[pl.ds(start, mixer_count), :], out_w[...], preferred_element_type=f32
        ).astype(bf16)

    for d in order:
        project(d, 1 - core, mix_twin)
        twin_mix(d).start()
    for d in order:
        project(d, core, mix_own)

    def mix_step(d, step):
        return to_tp(
            mix_own.at[d], (mix_right if step > 0 else mix_left).at[d], m_send.at[d],
            (m_right if step > 0 else m_left).at[d], (chip + step) * CORES + core,
        )

    def mix_wait(d, step):
        return to_tp(
            mix_own.at[d], (mix_right if step > 0 else mix_left).at[d], m_send.at[d],
            (m_right if step > 0 else m_left).at[d], twin,
        )

    def mix_lead(d):
        twin_mix(d).wait_recv()

        @pl.when((chip == 0) | (chip == chips - 1))
        def _():
            mix_own[d] = (mix_own[d].astype(f32) + mix_in[d].astype(f32)).astype(bf16)

        @pl.when(chip == 0)
        def _():
            mix_step(d, 1).start()

        @pl.when(chip == chips - 1)
        def _():
            mix_step(d, -1).start()

    def mix_follow(d):
        @pl.when((chip > 0) & (d > chip))
        def _():
            mix_wait(d, 1).wait_recv()
            mix_own[d] = (
                mix_own[d].astype(f32) + mix_in[d].astype(f32) + mix_right[d].astype(f32)
            ).astype(bf16)
            mix_step(d, 1).start()

        @pl.when((chip < chips - 1) & (d < chip))
        def _():
            mix_wait(d, -1).wait_recv()
            mix_own[d] = (
                mix_own[d].astype(f32) + mix_in[d].astype(f32) + mix_left[d].astype(f32)
            ).astype(bf16)
            mix_step(d, -1).start()

    def channel_step(d, step):
        return to_tp(
            channel.at[d], (channel_right if step > 0 else channel_left).at[d], c_send.at[d],
            (c_right if step > 0 else c_left).at[d], (chip + step) * CORES + core,
        )

    def channel_wait(d, step):
        return to_tp(
            channel.at[d], (channel_right if step > 0 else channel_left).at[d], c_send.at[d],
            (c_right if step > 0 else c_left).at[d], twin,
        )

    for d in order[:-1]:
        mix_lead(d)

    for q in near_first[1:]:
        take_row(q)

    for load in loads[5:]:
        load.wait()

    def twin_arrived(q):
        return to_tp(arrived.at[q, 0], arrived.at[q, 1], ta_send.at[q], ta_recv.at[q], twin)

    def twin_result(q):
        return to_tp(
            result_twin.at[q], result_in.at[q], ty_send.at[q], ty_recv.at[q], twin
        )

    def twin_shared(q):
        return to_tp(
            shared_twin.at[q], shared_in.at[q], th_send.at[q], th_recv.at[q], twin
        )

    def return_copy(q, k):
        target = flip(ep_index, k)
        return to_ep(
            result.at[q, target], returned.at[q, ep_index], r_send.at[q, k], r_recv.at[q, k],
            target,
        )

    def hand_over(q):
        for k in range(1, ep_count):
            dispatch_copy(q, k).wait_recv()
        twin_arrived(q).start()

    def gated_rows(rows, gate_weight, up_weight):
        gate_part = jnp.dot(rows, gate_weight, preferred_element_type=f32)
        up_part = jnp.dot(rows, up_weight, preferred_element_type=f32)
        return (gate_part / (1.0 + jnp.exp(-gate_part)) * up_part).astype(bf16)

    def shared(q):
        twin_row(q).wait_recv()
        rows = gathered[q].reshape(CORES * tokens_here, width)
        hidden = gated_rows(rows, sg[...], su[...])
        product = jnp.dot(hidden, sd[...], preferred_element_type=f32).astype(bf16)
        shared_own[q] = product[:tokens_here]
        shared_twin[q] = product[tokens_here:]
        twin_shared(q).start()

    def experts(q):
        twin_arrived(q).wait_recv()
        for j in range(local_experts):
            cut = slice(j * capacity, (j + 1) * capacity)
            rows = arrived[q, :, :, cut, :].reshape(CORES * ep_count * capacity, width)
            hidden = gated_rows(rows, eg[j], eu[j])
            product = jnp.dot(hidden, ed[j], preferred_element_type=f32).astype(bf16)
            product = product.reshape(CORES, ep_count, capacity, width)
            result[q, :, cut, :] = product[0]
            result_twin[q, :, cut, :] = product[1]
        twin_result(q).start()

    def give_back(q):
        twin_result(q).wait_recv()
        result[q] = (result[q].astype(f32) + result_in[q].astype(f32)).astype(bf16)
        for k in range(1, ep_count):
            return_copy(q, k).start()
        returned[q, ep_index] = result[q, ep_index]

    hand_over(order[0])
    for i, q in enumerate(order):
        shared(q)
        experts(q)
        if i + 1 < chips:
            hand_over(order[i + 1])
        give_back(q)
        if i == 1:
            mix_follow(order[0])

    def combined(q):
        for k in range(1, ep_count):
            return_copy(q, k).wait_recv()
        twin_shared(q).wait_recv()
        mixing = sum(
            jnp.where(
                notes[q][:, t : t + 1] == slot_lane, notes[q][:, topk + t : topk + t + 1], 0.0
            )
            for t in range(topk)
        )
        coarse = mixing.astype(bf16)
        fine = (mixing - coarse.astype(f32)).astype(bf16)
        rows = returned[q].reshape(slot_count, width)
        return (
            jnp.dot(coarse, rows, preferred_element_type=f32)
            + jnp.dot(fine, rows, preferred_element_type=f32)
            + shared_own[q].astype(f32)
            + shared_in[q].astype(f32)
        )

    def channel_on(d):
        own = combined(d)
        from_left = (chip > 0) & (d > chip)
        from_right = (chip < chips - 1) & (d < chip)

        @pl.when(from_left)
        def _():
            channel_wait(d, 1).wait_recv()
            channel[d] = (own + channel_right[d].astype(f32)).astype(bf16)

        @pl.when(from_right)
        def _():
            channel_wait(d, -1).wait_recv()
            channel[d] = (own + channel_left[d].astype(f32)).astype(bf16)

        @pl.when((chip == 0) | (chip == chips - 1))
        def _():
            channel[d] = own.astype(bf16)

        @pl.when(d > chip)
        def _():
            channel_step(d, 1).start()

        @pl.when(d < chip)
        def _():
            channel_step(d, -1).start()

    for i, d in enumerate(order[:-1]):
        channel_on(d)
        if i + 1 < chips - 1:
            mix_follow(order[i + 1])

    def line_end(own, right_step, left_step, right_buffer, left_buffer, out_ref):
        out_ref[...] = own.astype(out_ref.dtype)

        @pl.when((chip > 0) & (chip < chips - 1))
        def _():
            right_step.wait_recv()
            left_step.wait_recv()
            out_ref[...] = (
                own + right_buffer[chip].astype(f32) + left_buffer[chip].astype(f32)
            ).astype(out_ref.dtype)

        @pl.when(chip == chips - 1)
        def _():
            right_step.wait_recv()
            out_ref[...] = (own + right_buffer[chip].astype(f32)).astype(out_ref.dtype)

        @pl.when(chip == 0)
        def _():
            left_step.wait_recv()
            out_ref[...] = (own + left_buffer[chip].astype(f32)).astype(out_ref.dtype)

    twin_mix(chip).wait_recv()
    line_end(
        mix_own[chip].astype(f32) + mix_in[chip].astype(f32), mix_wait(chip, 1),
        mix_wait(chip, -1), mix_right, mix_left, mixer_ref,
    )
    line_end(
        combined(chip), channel_wait(chip, 1), channel_wait(chip, -1), channel_right,
        channel_left, channel_out_ref,
    )

    for d in order[:-1]:
        gather_row(chip, d).wait_send()
        gather_note(chip, d).wait_send()
        mix_wait(d, 1).wait_send()
        channel_wait(d, 1).wait_send()
    for q in range(chips):
        twin_row(q).wait_send()
        twin_mix(q).wait_send()
        twin_arrived(q).wait_send()
        twin_result(q).wait_send()
        twin_shared(q).wait_send()
        for k in range(1, ep_count):
            dispatch_copy(q, k).wait_send()
            return_copy(q, k).wait_send()
    for k in range(1, ep_count):
        state_copy(k).wait_send()
        total_copy(k).wait_send()


def turn_tables(key_width, sequence):
    half = key_width // 2
    inverse = np.float32(turn_base) ** (-np.arange(half, dtype=np.float32) / np.float32(half))
    inverse = inverse.astype(np.float64)

    def both(positions):
        angles = positions[:, None].astype(np.float64) * inverse[None, :]
        cosine, sine = np.cos(angles), np.sin(angles)
        return np.stack(
            [np.concatenate([cosine, cosine], axis=1), np.concatenate([-sine, sine], axis=1)]
        ).astype(np.float32)

    near = both(np.arange(BLOCK))
    far = both(np.arange(sequence // BLOCK) * BLOCK).transpose(1, 0, 2)
    return near, far


def whole_scratch(args, ep_count, chips, capacity):
    (
        query_rows, key_rows, value_rows, gate_rows, log_decay, out_weight, channel_input,
        _, _, _, expert_gate, expert_up, expert_down, shared_gate, shared_up, shared_down,
    ) = args
    f32, bf16 = jnp.float32, jnp.bfloat16
    tokens_here, width = channel_input.shape
    tokens, heads = query_rows.shape[0], log_decay.shape[0]
    key_width = query_rows.shape[1] // heads
    value_width = value_rows.shape[1] // heads
    blocks = tokens // BLOCK
    block_rows = expert_gate.shape[0] * capacity
    mixer_count = tokens // (chips * CORES)
    routed = (chips, ep_count, block_rows, width)
    rows = (chips, tokens_here, width)
    mixed = (chips, mixer_count, width)
    small = (8, 128)
    buffers = [(a.shape, a.dtype) for a in (
        query_rows, key_rows, value_rows, gate_rows, out_weight, expert_gate, expert_up,
        expert_down, shared_gate, shared_up, shared_down,
    )]
    buffers += [
        ((chips, CORES, tokens_here, width), bf16), ((chips, tokens_here, 128), f32),
        (routed, bf16), ((chips, CORES) + routed[1:], bf16), (routed, bf16), (routed, bf16),
        (routed, bf16), (routed, bf16),
    ]
    buffers += [(rows, bf16)] * 6 + [(mixed, bf16)] * 5
    buffers += [
        (value_rows.shape, bf16), (key_rows.shape, bf16),
        ((blocks, heads, key_width, value_width), f32), ((heads, key_width, value_width), f32),
        ((heads, key_width, value_width), bf16),
        ((ep_count, heads, key_width, value_width), bf16), (small, f32),
        ((ep_count,) + small, f32), ((blocks,) + small, f32), ((blocks * heads, BLOCK), f32),
        ((blocks, 8, BLOCK), f32), ((blocks, BLOCK, 128), f32),
        ((heads, key_width, value_width), f32),
    ]
    one, two, by_ep = (chips,), (chips, ep_count), (ep_count,)
    counts = [(11,)] + [one] * 6 + [two] * 2 + [one] * 6 + [two] * 2 + [by_ep] * 4 + [one] * 8
    return buffers, counts


def whole_step(args, ep_count, chips, capacity):
    (
        query_rows, key_rows, value_rows, gate_rows, log_decay, out_weight, channel_input,
        norm_gain, routes, route_weight, expert_gate, expert_up, expert_down, shared_gate,
        shared_up, shared_down,
    ) = args
    tokens_here, width = channel_input.shape
    tokens, heads = query_rows.shape[0], log_decay.shape[0]
    mixer_count = tokens // (chips * CORES)
    near, far = turn_tables(query_rows.shape[1] // heads, tokens * ep_count)
    buffers, counts = whole_scratch(args, ep_count, chips, capacity)
    vmem = pl.BlockSpec(memory_space=pltpu.VMEM)
    hbm = pl.BlockSpec(memory_space=pl.ANY)
    return pl.pallas_call(
        functools.partial(whole_kernel, (ep_count, chips, capacity)),
        out_shape=(
            jax.ShapeDtypeStruct((mixer_count, width), jnp.bfloat16),
            jax.ShapeDtypeStruct((tokens_here, width), jnp.bfloat16),
        ),
        in_specs=[vmem] * 7 + [hbm] * 11,
        out_specs=(vmem, vmem),
        scratch_shapes=[pltpu.VMEM(shape, dtype) for shape, dtype in buffers]
        + [pltpu.SemaphoreType.DMA(count) for count in counts],
        compiler_params=pltpu.CompilerParams(
            collective_id=0, has_side_effects=True, vmem_limit_bytes=KERNEL_VMEM
        ),
    )(
        channel_input, norm_gain.reshape(1, width), routes, route_weight, log_decay,
        jnp.asarray(near), jnp.asarray(far), query_rows, key_rows, value_rows, gate_rows,
        out_weight, expert_gate, expert_up, expert_down, shared_gate, shared_up, shared_down,
    )


def padded_bytes(shape, dtype):
    size = jnp.dtype(dtype).itemsize
    rows = 32 // size
    last = -(-shape[-1] // 128) * 128
    return math.prod(shape[:-2]) * (-(-shape[-2] // rows) * rows) * last * size


def one_kernel_fits(args, ep_count, chips, capacity):
    query_rows, log_decay, experts = args[0], args[4], args[10].shape[0] * ep_count
    heads = log_decay.shape[0]
    buffers, _ = whole_scratch(args, ep_count, chips, capacity)
    need = sum(padded_bytes(shape, dtype) for shape, dtype in buffers)
    return (
        chips > 1
        and capacity % 16 == 0
        and experts <= 128
        and heads <= 8
        and query_rows.shape[1] // heads == 128
        and args[6].shape[0] % 16 == 0
        and need <= KERNEL_VMEM - (10 << 20)
    )


def local(
    query_rows, key_rows, value_rows, gate_rows, log_decay, out_weight, channel_input, norm_gain,
    routes, route_weight, expert_gate, expert_up, expert_down, shared_gate, shared_up, shared_down,
):
    ep_count, tp_count = lax.axis_size("ep"), lax.axis_size("tp")
    ep_index, tp_index = lax.axis_index("ep"), lax.axis_index("tp")
    chips = tp_count // CORES
    chip, core = tp_index // CORES, tp_index % CORES
    tokens_here, width = channel_input.shape
    topk = routes.shape[1]
    local_experts = expert_gate.shape[0]
    experts_all = ep_count * local_experts
    capacity = tokens_here * topk // experts_all + max(
        2, tokens_here * topk // (3 * experts_all)
    )

    args = (
        query_rows, key_rows, value_rows, gate_rows, log_decay, out_weight, channel_input,
        norm_gain, routes, route_weight, expert_gate, expert_up, expert_down, shared_gate,
        shared_up, shared_down,
    )
    if one_kernel_fits(args, ep_count, chips, capacity):
        return whole_step(args, ep_count, chips, capacity)

    wide = channel_input.astype(jnp.float32)
    normed = (
        wide * lax.rsqrt(jnp.mean(wide * wide, axis=-1, keepdims=True) + epsilon) * norm_gain
    ).astype(jnp.bfloat16)
    flat = routes.reshape(-1)
    onehot = (flat[:, None] == jnp.arange(experts_all, dtype=jnp.int32)[None, :]).astype(
        jnp.float32
    )
    count = tokens_here * topk
    before = (jnp.arange(count)[:, None] > jnp.arange(count)[None, :]).astype(jnp.float32)
    rank = jnp.sum(jnp.dot(before, onehot) * onehot, axis=1)
    notes = jnp.concatenate(
        [routes.astype(jnp.float32), rank.reshape(tokens_here, topk), route_weight], axis=1
    )
    notes = jnp.pad(notes, ((0, 0), (0, 128 - 3 * topk)))
    own_rows = line_gather(normed, chips)
    notes_all = line_gather(notes, chips)
    log_decay, normed, notes = lax.optimization_barrier((log_decay, normed, notes))
    route_all = notes_all[:, :, :topk].astype(jnp.int32)
    rank_all = notes_all[:, :, topk : 2 * topk].astype(jnp.int32)
    weight_all = notes_all[:, :, 2 * topk : 3 * topk]
    place = jnp.arange(chips, dtype=jnp.int32)[:, None, None]
    turn = (route_all // local_experts) ^ ep_index
    slot = ((turn * local_experts + route_all % local_experts) * chips + place) * capacity
    slot = (slot + rank_all).reshape(chips * tokens_here, topk)
    slot_count = experts_all * chips * capacity
    slot_ids = jnp.arange(slot_count, dtype=jnp.int32)
    placing = sum(
        (slot_ids[:, None] == slot[None, :, t]).astype(jnp.bfloat16) for t in range(topk)
    )
    own_flat = own_rows.reshape(chips * tokens_here, width)
    outgoing = jnp.dot(placing, own_flat, preferred_element_type=jnp.float32).astype(jnp.bfloat16)
    outgoing = outgoing.reshape(ep_count, local_experts, chips * capacity, width)
    arrived = [outgoing[0]] + [swap_ep(outgoing[k], k, ep_count) for k in range(1, ep_count)]
    own_twin = swap_cores(own_flat, tp_count)

    gated = retention(query_rows, key_rows, value_rows, gate_rows, log_decay)
    mixer_count = query_rows.shape[0] // tp_count
    gated_parts = gated.reshape(chips, CORES, mixer_count, gated.shape[1])

    def mixer_for(which):
        mine = lax.dynamic_index_in_dim(gated_parts, which, 1, keepdims=False)
        product = jnp.dot(
            mine.reshape(chips * mixer_count, -1), out_weight, preferred_element_type=jnp.float32
        )
        return product.astype(jnp.bfloat16)

    mixer_twin, mixer_mine = mixer_for(1 - core), mixer_for(core)
    mixer_half = summed(mixer_mine, swap_cores(mixer_twin, tp_count))
    arrived, _ = lax.optimization_barrier((arrived, (mixer_twin, mixer_mine)))
    arrived_twin = [swap_cores(block, tp_count) for block in arrived]
    mixer_half = mixer_half.reshape(chips, mixer_count, width)
    mixer_out = line_scatter(
        lambda r: lax.dynamic_index_in_dim(mixer_half, (chip + r) % chips, 0, False), chips
    ).astype(jnp.bfloat16)

    def experts_on(blocks, rows):
        routed = jnp.concatenate(blocks, axis=1)
        gate_part = jnp.einsum("emd,edf->emf", routed, expert_gate, preferred_element_type=jnp.float32)
        up_part = jnp.einsum("emd,edf->emf", routed, expert_up, preferred_element_type=jnp.float32)
        hidden = gated_pair(gate_part, up_part)
        routed_term = jnp.einsum(
            "emf,efd->emd", hidden, expert_down, preferred_element_type=jnp.float32
        ).astype(jnp.bfloat16)
        shared_hidden = gated_pair(
            jnp.dot(rows, shared_gate, preferred_element_type=jnp.float32),
            jnp.dot(rows, shared_up, preferred_element_type=jnp.float32),
        )
        shared_term = jnp.dot(
            shared_hidden, shared_down, preferred_element_type=jnp.float32
        ).astype(jnp.bfloat16)
        return routed_term, shared_term

    routed_twin, shared_twin = experts_on(arrived_twin, own_twin)
    routed_mine, shared_mine = experts_on(arrived, own_flat)
    routed = summed(routed_mine, swap_cores(routed_twin, tp_count))
    shared = summed(shared_mine, swap_cores(shared_twin, tp_count))
    routed = routed.reshape(local_experts, ep_count, chips * capacity, width)
    returned = [routed[:, 0]] + [swap_ep(routed[:, k], k, ep_count) for k in range(1, ep_count)]
    returned = jnp.stack(returned).reshape(slot_count, width)
    flat_weight = weight_all.reshape(chips * tokens_here, topk)
    mixing = sum(
        jnp.where(slot_ids[None, :] == slot[:, t : t + 1], flat_weight[:, t : t + 1], 0.0)
        for t in range(topk)
    )
    coarse = lax.reduce_precision(mixing, 8, 7)
    fine = (mixing - coarse).astype(jnp.bfloat16)
    coarse = coarse.astype(jnp.bfloat16)
    channel = (
        jnp.dot(coarse, returned, preferred_element_type=jnp.float32)
        + jnp.dot(fine, returned, preferred_element_type=jnp.float32)
        + shared.astype(jnp.float32)
    ).astype(jnp.bfloat16)
    channel = channel.reshape(chips, tokens_here, width)
    channel_out = line_scatter(lambda r: channel[(chips - r) % chips], chips).astype(jnp.bfloat16)
    return (mixer_out, channel_out)


def solution(mesh):
    in_specs = (
        P("ep", "tp"),
        P("ep", "tp"),
        P("ep", "tp"),
        P("ep", "tp"),
        P("tp", "ep"),
        P("tp", None),
        P(("ep", "tp"), None),
        P(),
        P(("ep", "tp"), None),
        P(("ep", "tp"), None),
        P("ep", None, "tp"),
        P("ep", None, "tp"),
        P("ep", "tp", None),
        P(None, "tp"),
        P(None, "tp"),
        P("tp", None),
    )
    out_specs = (P(("ep", "tp"), None), P(("ep", "tp"), None))
    return jax.shard_map(local, mesh=mesh, in_specs=in_specs, out_specs=out_specs, check_vma=False)
```

```python
import functools
import math

import jax
import jax.numpy as jnp
import numpy as np
from jax import lax
from jax.experimental import pallas as pl
from jax.experimental.pallas import tpu as pltpu
from jax.sharding import PartitionSpec as P

BLOCK = 128
CORES = 2
KERNEL_VMEM = 67043328

epsilon = 1e-06
turn_base = 10000.0


def shift_chips(array, r, count):
    pairs = [
        (z * CORES + c, (z + r) % count * CORES + c) for z in range(count) for c in range(CORES)
    ]
    return lax.ppermute(array, "tp", pairs)


def line_gather(array, count):
    return jnp.stack([array] + [shift_chips(array, r, count) for r in range(1, count)])


def line_scatter(part, count):
    total = part(0).astype(jnp.float32)
    for r in range(1, count):
        total = total + shift_chips(part(r), r, count).astype(jnp.float32)
    return total


def swap_cores(array, tp_count):
    return lax.ppermute(array, "tp", [(i, i ^ 1) for i in range(tp_count)])


def swap_ep(array, k, ep_count):
    return lax.ppermute(array, "ep", [(i, i ^ k) for i in range(ep_count)])


def turned(rows, cosine, sine):
    wide = rows.astype(jnp.float32)
    return (wide * cosine + pltpu.roll(wide, wide.shape[1] // 2, 1) * sine).astype(jnp.bfloat16)


def state_kernel(key_ref, value_ref, cosine_ref, sine_ref, fade_ref, state_ref):
    heads, key_width, value_width = state_ref.shape
    for h in range(heads):
        keys = turned(
            key_ref[:, h * key_width : (h + 1) * key_width], cosine_ref[...], sine_ref[...]
        )
        faded = (keys.astype(jnp.float32) * fade_ref[:, h : h + 1]).astype(jnp.bfloat16)
        state_ref[h] = lax.dot_general(
            faded,
            value_ref[:, h * value_width : (h + 1) * value_width],
            (((0,), (0,)), ((), ())),
            preferred_element_type=jnp.float32,
        ).astype(state_ref.dtype)


def retention_kernel(
    query_ref, key_ref, value_ref, gate_ref, cosine_ref, sine_ref, column_ref, row_ref,
    entry_ref, out_ref, state,
):
    heads, key_width, value_width = state.shape

    @pl.when(pl.program_id(0) == 0)
    def _():
        state[...] = entry_ref[...]

    cosine, sine = cosine_ref[...], sine_ref[...]
    lower = lax.broadcasted_iota(jnp.int32, (BLOCK, BLOCK), 0) >= lax.broadcasted_iota(
        jnp.int32, (BLOCK, BLOCK), 1
    )
    for h in range(heads):
        key_cut = slice(h * key_width, (h + 1) * key_width)
        value_cut = slice(h * value_width, (h + 1) * value_width)
        queries = turned(query_ref[:, key_cut], cosine, sine)
        keys = turned(key_ref[:, key_cut], cosine, sine)
        values = value_ref[:, value_cut]
        column = column_ref[:, h : h + 1]
        row = row_ref[0, h : h + 1, :]
        end = column_ref[BLOCK - 1 : BLOCK, h : h + 1]
        scores = lax.dot_general(
            queries, keys, (((1,), (1,)), ((), ())), preferred_element_type=jnp.float32
        )
        spread = jnp.exp(jnp.where(lower, column - row, 0.0))
        weights = jnp.where(lower, scores * spread, 0.0).astype(jnp.bfloat16)
        before = state[h]
        retained = jnp.dot(weights, values, preferred_element_type=jnp.float32)
        retained = retained + jnp.exp(column) * jnp.dot(
            queries, before.astype(jnp.bfloat16), preferred_element_type=jnp.float32
        )
        faded = (keys.astype(jnp.float32) * jnp.exp(end - column)).astype(jnp.bfloat16)
        state[h] = jnp.exp(end) * before + lax.dot_general(
            faded, values, (((0,), (0,)), ((), ())), preferred_element_type=jnp.float32
        )
        scale = lax.rsqrt(jnp.mean(retained * retained, axis=1, keepdims=True) + epsilon)
        gate = gate_ref[:, value_cut].astype(jnp.float32)
        out_ref[:, value_cut] = (gate / (1.0 + jnp.exp(-gate)) * (retained * scale)).astype(
            jnp.bfloat16
        )


def retention(query_rows, key_rows, value_rows, gate_rows, log_decay):
    tokens = query_rows.shape[0]
    heads = log_decay.shape[0]
    key_width = query_rows.shape[1] // heads
    value_width = value_rows.shape[1] // heads
    blocks = tokens // BLOCK
    ep_count, ep_index = lax.axis_size("ep"), lax.axis_index("ep")
    half = key_width // 2
    position = (ep_index * tokens + jnp.arange(tokens, dtype=jnp.int32)).astype(jnp.float32)
    inverse = turn_base ** (-jnp.arange(half, dtype=jnp.float32) / half)
    angles = position[:, None] * inverse[None, :]
    cosine, sine = jnp.cos(angles), jnp.sin(angles)
    cosine = jnp.concatenate([cosine, cosine], axis=1)
    sine = jnp.concatenate([-sine, sine], axis=1)
    running = jnp.cumsum(log_decay.reshape(heads, blocks, BLOCK), axis=2)
    ends = running[:, :, -1]
    later = jnp.sum(ends, axis=1, keepdims=True) - jnp.cumsum(ends, axis=1)
    later = jnp.minimum(later, 0.0)
    fade = jnp.exp(ends[:, :, None] - running + later[:, :, None]).reshape(heads, tokens).T
    total = jnp.sum(ends, axis=1)
    vmem = pl.BlockSpec(memory_space=pltpu.VMEM)
    own_state = pl.pallas_call(
        state_kernel,
        out_shape=jax.ShapeDtypeStruct((heads, key_width, value_width), jnp.bfloat16),
        in_specs=[vmem] * 5,
        out_specs=vmem,
        cost_estimate=pl.CostEstimate(
            flops=2 * tokens * heads * key_width * value_width * 4,
            bytes_accessed=8 << 20,
            transcendentals=0,
        ),
    )(key_rows, value_rows, cosine, sine, fade)
    totals_sent = jnp.broadcast_to(total[:, None], (heads, 128))
    states, totals = [], [total]
    for k in range(1, ep_count):
        states.append(swap_ep(own_state, k, ep_count))
        totals.append(swap_ep(totals_sent, k, ep_count)[:, 0])
    entry = jnp.zeros((heads, key_width, value_width), jnp.float32)
    for k in range(1, ep_count):
        source = ep_index ^ k
        passed = jnp.zeros_like(total)
        for m in range(1, ep_count):
            between = ((ep_index ^ m) > source) & ((ep_index ^ m) < ep_index)
            passed = passed + jnp.where(between, totals[m], 0.0)
        share = jnp.where(source < ep_index, jnp.exp(passed), 0.0)
        entry = entry + share[:, None, None] * states[k - 1].astype(jnp.float32)
    columns = running.reshape(heads, tokens).T
    rows = running.transpose(1, 0, 2)
    by_block = lambda width: pl.BlockSpec((BLOCK, width), lambda n: (n, 0))
    whole = pl.BlockSpec((heads, key_width, value_width), lambda n: (0, 0, 0))
    return pl.pallas_call(
        retention_kernel,
        out_shape=jax.ShapeDtypeStruct((tokens, heads * value_width), jnp.bfloat16),
        grid=(blocks,),
        in_specs=[
            by_block(heads * key_width),
            by_block(heads * key_width),
            by_block(heads * value_width),
            by_block(heads * value_width),
            by_block(key_width),
            by_block(key_width),
            by_block(heads),
            pl.BlockSpec((1, heads, BLOCK), lambda n: (n, 0, 0)),
            whole,
        ],
        out_specs=by_block(heads * value_width),
        scratch_shapes=[pltpu.VMEM((heads, key_width, value_width), jnp.float32)],
        cost_estimate=pl.CostEstimate(
            flops=8 << 30, bytes_accessed=24 << 20, transcendentals=0
        ),
    )(query_rows, key_rows, value_rows, gate_rows, cosine, sine, columns, rows, entry)


def gated_pair(gate_part, up_part):
    return (jax.nn.silu(gate_part) * up_part).astype(jnp.bfloat16)


def summed(a, b):
    return (a.astype(jnp.float32) + b.astype(jnp.float32)).astype(jnp.bfloat16)


def flip(index, k):
    turned_index, bit = index, 1
    while bit <= k:
        if k & bit:
            turned_index = turned_index + bit - 2 * bit * ((index // bit) % 2)
        bit *= 2
    return turned_index


def line_order(chips):
    orders = []
    for z in range(chips):
        right, left = list(range(chips - 1, z, -1)), list(range(z))
        order = []
        while right or left:
            if len(right) >= len(left) and right:
                order.append(right.pop(0))
            elif left:
                order.append(left.pop(0))
        orders.append(order + [z])
    return orders


def arrival_order(chips):
    def rank(z, q):
        hands_on = (q <= z - 2 and z < chips - 1) or (q >= z + 2 and z > 0)
        return (not hands_on, abs(q - z), q)

    return [
        sorted((q for q in range(chips) if q != z), key=functools.partial(rank, z))
        for z in range(chips)
    ]


def pick(table, index):
    chosen = 0
    for i, entry in enumerate(table):
        chosen = chosen + jnp.where(index == i, entry, 0)
    return chosen


def in_steps(count, together, body):
    together = math.gcd(count, together)

    def step(i, carry):
        for j in range(together):
            body(i * together + j)
        return carry

    lax.fori_loop(0, count // together, step, 0)


def whole_kernel(
    sizes,
    channel_ref, gain_ref, routes_ref, weight_ref, decay_ref, near_ref, far_ref,
    query_any, key_any, value_any, gate_any, out_any, eg_any, eu_any, ed_any, sg_any, su_any,
    sd_any,
    mixer_ref, channel_out_ref,
    query, key, value, gate, out_w, eg, eu, ed, sg, su, sd,
    gathered, slots, arrived, result_twin, result_in, result, returned,
    shared_twin, shared_in, shared_own, channel, channel_right, channel_left,
    mix_twin, mix_in, mix_own, mix_right, mix_left,
    gated, partial, keys_turned, before, entry, state_send, state_in, total_send, total_in, prefix,
    decay_flat, run_row, run_col,
    local_sem, g_send, g_recv, f_send, tg_send, tg_recv, d_send, d_recv, ta_send, ta_recv,
    ty_send, ty_recv, th_send, th_recv, r_send, r_recv, s_send, s_recv, o_send, o_recv,
    tp_send, tp_recv, m_send, m_right, m_left, c_send, c_right, c_left,
):
    ep_count, chips, capacity = sizes
    f32, bf16 = jnp.float32, jnp.bfloat16
    tokens_here, width = channel_ref.shape
    topk = routes_ref.shape[0]
    local_experts = eg.shape[0]
    block_rows = local_experts * capacity
    slot_count = ep_count * block_rows
    heads, key_width, value_width = entry.shape
    blocks = before.shape[0]
    mixer_count = mixer_ref.shape[0]
    ep_index, tp_index = lax.axis_index("ep"), lax.axis_index("tp")
    chip, core = tp_index // CORES, tp_index % CORES
    twin = tp_index + 1 - 2 * core
    orders = line_order(chips)
    order = [pick([row[i] for row in orders], chip) for i in range(chips - 1)] + [chip]
    arrivals = arrival_order(chips)
    arrival = [pick([row[i] for row in arrivals], chip) for i in range(chips - 1)]

    def to_tp(src, dst, send, recv, target):
        return pltpu.make_async_remote_copy(
            src_ref=src, dst_ref=dst, send_sem=send, recv_sem=recv,
            device_id={"tp": target}, device_id_type=pl.DeviceIdType.MESH,
        )

    def to_ep(src, dst, send, recv, target):
        return pltpu.make_async_remote_copy(
            src_ref=src, dst_ref=dst, send_sem=send, recv_sem=recv,
            device_id={"ep": target}, device_id_type=pl.DeviceIdType.MESH,
        )

    barrier = pltpu.get_barrier_semaphore()
    for r in range(1, chips):
        pl.semaphore_signal(
            barrier, inc=1, device_id={"tp": (chip + r) % chips * CORES + core},
            device_id_type=pl.DeviceIdType.MESH,
        )
    pl.semaphore_signal(
        barrier, inc=1, device_id={"tp": twin}, device_id_type=pl.DeviceIdType.MESH
    )
    for k in range(1, ep_count):
        pl.semaphore_signal(
            barrier, inc=1, device_id={"ep": flip(ep_index, k)},
            device_id_type=pl.DeviceIdType.MESH,
        )

    pairs = [
        (key_any, key), (value_any, value), (query_any, query), (gate_any, gate),
        (out_any, out_w), (sg_any, sg), (su_any, su), (sd_any, sd), (eg_any, eg), (eu_any, eu),
        (ed_any, ed),
    ]
    loads = [pltpu.make_async_copy(s, d, local_sem.at[i]) for i, (s, d) in enumerate(pairs)]
    for load in loads:
        load.start()

    wide = channel_ref[...].astype(f32)
    normed = (
        wide * lax.rsqrt(jnp.mean(wide * wide, axis=-1, keepdims=True) + epsilon) * gain_ref[...]
    ).astype(bf16)
    gathered[chip, 0, :, :width] = normed
    lane = lax.broadcasted_iota(jnp.int32, (tokens_here, 128), 1)
    same = (
        lax.broadcasted_iota(jnp.int32, (tokens_here, tokens_here), 0)
        == lax.broadcasted_iota(jnp.int32, (tokens_here, tokens_here), 1)
    ).astype(f32)

    def as_columns(rows):
        return lax.dot_general(
            same, rows, (((1,), (1,)), ((), ())), preferred_element_type=f32,
            precision=lax.Precision.HIGHEST,
        )

    route_columns = as_columns(routes_ref[...].astype(f32))
    weight_columns = as_columns(weight_ref[...])
    routed_to = [route_columns[:, t : t + 1] for t in range(topk)]
    named = [(route == lane.astype(f32)).astype(f32) for route in routed_to]
    earlier = (
        lax.broadcasted_iota(jnp.int32, (tokens_here, tokens_here), 0)
        > lax.broadcasted_iota(jnp.int32, (tokens_here, tokens_here), 1)
    ).astype(bf16)
    ahead = jnp.dot(earlier, sum(named).astype(bf16), preferred_element_type=f32)
    noted = jnp.zeros((tokens_here, 128), f32)
    for t in range(topk):
        rank = jnp.sum(ahead * named[t], axis=1, keepdims=True)
        noted = jnp.where(lane == t, routed_to[t] * capacity + rank, noted)
        left = weight_columns[:, t : t + 1]
        for piece in range(3):
            term = left.astype(bf16).astype(f32)
            noted = jnp.where(lane == topk + 3 * t + piece, term, noted)
            left = left - term
    gathered[chip, 0, :, width:] = noted.astype(bf16)

    def slot_of(q, t):
        return gathered[q, 0, :, width:].astype(f32)[:, t : t + 1]

    def weight_of(q, t):
        terms = gathered[q, 0, :, width:].astype(f32)
        at = topk + 3 * t
        return terms[:, at : at + 1] + terms[:, at + 1 : at + 2] + terms[:, at + 2 : at + 3]

    pl.semaphore_wait(barrier, chips + ep_count - 1)

    def gather_row(q, target):
        return to_tp(
            gathered.at[q, 0], gathered.at[q, 0], g_send.at[target], g_recv.at[q],
            target * CORES + core,
        )

    def relay_row(q, target):
        return to_tp(
            gathered.at[q, 0], gathered.at[q, 0], f_send.at[q], g_recv.at[q],
            target * CORES + core,
        )

    def relay(q, act):
        @pl.when((q <= chip - 2) & (chip < chips - 1))
        def _():
            act(relay_row(q, chip + 1))

        @pl.when((q >= chip + 2) & (chip > 0))
        def _():
            act(relay_row(q, chip - 1))

    def twin_row(q):
        return to_tp(
            gathered.at[q, 0], gathered.at[q, 1], tg_send.at[q], tg_recv.at[q], twin
        )

    def reached(target):
        return (target - chip) * (target - chip) <= 4

    for target in order[:-1]:
        @pl.when(reached(target))
        def _():
            gather_row(chip, target).start()

    twin_row(chip).start()

    slot_lane = lax.broadcasted_iota(jnp.int32, (tokens_here, slot_count), 1).astype(f32)

    def dispatch_copy(q, k):
        target = flip(ep_index, k)
        return to_ep(
            slots.at[q, target], arrived.at[q, 0, ep_index], d_send.at[q, k], d_recv.at[q, k],
            target,
        )

    def dispatch(q):
        placing = sum(
            (slot_of(q, t) == slot_lane).astype(f32) for t in range(topk)
        ).astype(bf16)
        rows = lax.dot_general(
            placing, gathered[q, 0, :, :width], (((0,), (0,)), ((), ())), preferred_element_type=f32
        ).astype(bf16)
        slots[q] = rows.reshape(ep_count, block_rows, width)
        for k in range(1, ep_count):
            dispatch_copy(q, k).start()
        arrived[q, 0, ep_index] = slots[q, ep_index]

    def take_row(q):
        gather_row(q, q).wait_recv()
        relay(q, lambda copy: copy.start())
        twin_row(q).start()
        dispatch(q)

    for n in range(blocks):
        decay_flat[n * heads : (n + 1) * heads, :] = decay_ref[:, n * BLOCK : (n + 1) * BLOCK]
    upper = (
        lax.broadcasted_iota(jnp.int32, (BLOCK, BLOCK), 0)
        <= lax.broadcasted_iota(jnp.int32, (BLOCK, BLOCK), 1)
    )
    lower = (
        lax.broadcasted_iota(jnp.int32, (BLOCK, BLOCK), 0)
        >= lax.broadcasted_iota(jnp.int32, (BLOCK, BLOCK), 1)
    )
    flat = decay_flat[...]
    by_row = jnp.dot(
        flat, upper.astype(f32), preferred_element_type=f32, precision=lax.Precision.HIGHEST
    )
    by_col = lax.dot_general(
        lower.astype(f32), flat, (((1,), (1,)), ((), ())), preferred_element_type=f32,
        precision=lax.Precision.HIGHEST,
    )
    for n in range(blocks):
        run_row[n] = jnp.zeros(run_row.shape[1:], f32)
        run_row[n, 0:heads, :] = by_row[n * heads : (n + 1) * heads, :]
        run_col[n, :, 0:heads] = by_col[:, n * heads : (n + 1) * heads]

    def turns(n):
        far = far_ref[ep_index * blocks + n]
        far_cos, far_sin = far[0:1, :], far[1:2, :]
        near_cos, near_sin = near_ref[0], near_ref[1]
        return near_cos * far_cos - near_sin * far_sin, near_sin * far_cos + near_cos * far_sin

    whole_decay = jnp.zeros(total_send.shape, f32)
    for n in range(blocks):
        prefix[n] = whole_decay
        whole_decay = whole_decay + run_row[n, :, BLOCK - 1 : BLOCK]
    total_send[...] = whole_decay

    def state_copy(k, h):
        return to_ep(
            state_send.at[h], state_in.at[k, h], s_send.at[k, h], s_recv.at[k, h],
            flip(ep_index, k),
        )

    def total_copy(k):
        return to_ep(
            total_send, total_in.at[k], o_send.at[k], o_recv.at[k], flip(ep_index, k)
        )

    for k in range(1, ep_count):
        @pl.when(flip(ep_index, k) > ep_index)
        def _():
            total_copy(k).start()

    loads[0].wait()
    loads[1].wait()

    def first_pass(h):
        key_cut = slice(h * key_width, (h + 1) * key_width)
        value_cut = slice(h * value_width, (h + 1) * value_width)
        held = jnp.zeros((key_width, value_width), f32)
        for n in range(blocks):
            at = slice(n * BLOCK, (n + 1) * BLOCK)
            keys = turned(key[at, key_cut], *turns(n))
            keys_turned[at, key_cut] = keys
            end = run_row[n, h : h + 1, BLOCK - 1 : BLOCK]
            faded = (keys.astype(f32) * jnp.exp(end - run_col[n, :, h : h + 1])).astype(bf16)
            before[n, h] = held
            held = jnp.exp(end) * held + lax.dot_general(
                faded, value[at, value_cut], (((0,), (0,)), ((), ())),
                preferred_element_type=f32,
            )
        state_send[h] = held.astype(bf16)

    for h in range(heads):
        first_pass(h)
        for k in range(1, ep_count):
            @pl.when(flip(ep_index, k) > ep_index)
            def _():
                state_copy(k, h).start()

    dispatch(chip)

    loads[2].wait()

    def second_pass(n):
        at = pl.ds(pl.multiple_of(n * BLOCK, BLOCK), BLOCK)
        cosine, sine = turns(n)
        for h in range(heads):
            key_cut = slice(h * key_width, (h + 1) * key_width)
            value_cut = slice(h * value_width, (h + 1) * value_width)
            queries = turned(query[at, key_cut], cosine, sine)
            query[at, key_cut] = queries
            column = run_col[n, :, h : h + 1]
            row = run_row[n, h : h + 1, :]
            scores = lax.dot_general(
                queries, keys_turned[at, key_cut], (((1,), (1,)), ((), ())),
                preferred_element_type=f32,
            )
            spread = jnp.exp(jnp.where(lower, column - row, 0.0))
            weights = jnp.where(lower, scores * spread, 0.0).astype(bf16)
            partial[at, value_cut] = jnp.dot(
                weights, value[at, value_cut], preferred_element_type=f32
            ) + jnp.exp(column) * jnp.dot(
                queries, before[n, h].astype(bf16), preferred_element_type=f32
            )

    in_steps(blocks, 2, second_pass)

    loads[3].wait()
    for k in range(1, ep_count):
        @pl.when(flip(ep_index, k) < ep_index)
        def _():
            total_copy(k).wait_recv()

        @pl.when(flip(ep_index, k) > ep_index)
        def _():
            total_in[k] = jnp.zeros_like(total_send)
            state_in[k] = jnp.zeros_like(state_send)

    shares = []
    for k in range(1, ep_count):
        source = flip(ep_index, k)
        passed = jnp.zeros(total_send.shape, f32)
        for m in range(1, ep_count):
            between = (flip(ep_index, m) > source) & (flip(ep_index, m) < ep_index)
            passed = passed + jnp.where(between, total_in[m], 0.0)
        shares.append(jnp.where(source < ep_index, jnp.exp(passed), 0.0))

    def third_pass(h):
        for k in range(1, ep_count):
            @pl.when(flip(ep_index, k) < ep_index)
            def _():
                state_copy(k, h).wait_recv()

        entry[h] = sum(
            shares[k - 1][h : h + 1, 0:1] * state_in[k, h].astype(f32)
            for k in range(1, ep_count)
        )
        value_cut = slice(h * value_width, (h + 1) * value_width)

        def finish(n):
            at = pl.ds(pl.multiple_of(n * BLOCK, BLOCK), BLOCK)
            grown = jnp.exp(run_col[n, :, h : h + 1] + prefix[n, h : h + 1, 0:1])
            retained = partial[at, value_cut] + grown * jnp.dot(
                query[at, h * key_width : (h + 1) * key_width], entry[h].astype(bf16),
                preferred_element_type=f32,
            )
            scale = lax.rsqrt(jnp.mean(retained * retained, axis=1, keepdims=True) + epsilon)
            gates = gate[at, value_cut].astype(f32)
            gated[at, value_cut] = (
                gates / (1.0 + jnp.exp(-gates)) * (retained * scale)
            ).astype(bf16)

        in_steps(blocks, 4, finish)

    for h in range(heads):
        third_pass(h)

    loads[4].wait()

    def twin_mix(d):
        return to_tp(mix_twin.at[d], mix_in.at[d], tp_send.at[d], tp_recv.at[d], twin)

    def project(d, which, into):
        start = pl.multiple_of((d * CORES + which) * mixer_count, mixer_count)
        into[d] = jnp.dot(
            gated[pl.ds(start, mixer_count), :], out_w[...], preferred_element_type=f32
        ).astype(bf16)

    def mix_step(d, step):
        return to_tp(
            mix_own.at[d], (mix_right if step > 0 else mix_left).at[d], m_send.at[d],
            (m_right if step > 0 else m_left).at[d], (chip + step) * CORES + core,
        )

    def mix_wait(d, step):
        return to_tp(
            mix_own.at[d], (mix_right if step > 0 else mix_left).at[d], m_send.at[d],
            (m_right if step > 0 else m_left).at[d], twin,
        )

    def mix_lead(d):
        twin_mix(d).wait_recv()

        @pl.when((chip == 0) | (chip == chips - 1))
        def _():
            mix_own[d] = (mix_own[d].astype(f32) + mix_in[d].astype(f32)).astype(bf16)

        @pl.when(chip == 0)
        def _():
            mix_step(d, 1).start()

        @pl.when(chip == chips - 1)
        def _():
            mix_step(d, -1).start()

    def mix_follow(d):
        @pl.when((chip > 0) & (d > chip))
        def _():
            mix_wait(d, 1).wait_recv()
            mix_own[d] = (
                mix_own[d].astype(f32) + mix_in[d].astype(f32) + mix_right[d].astype(f32)
            ).astype(bf16)
            mix_step(d, 1).start()

        @pl.when((chip < chips - 1) & (d < chip))
        def _():
            mix_wait(d, -1).wait_recv()
            mix_own[d] = (
                mix_own[d].astype(f32) + mix_in[d].astype(f32) + mix_left[d].astype(f32)
            ).astype(bf16)
            mix_step(d, -1).start()

    def channel_step(d, step):
        return to_tp(
            channel.at[d], (channel_right if step > 0 else channel_left).at[d], c_send.at[d],
            (c_right if step > 0 else c_left).at[d], (chip + step) * CORES + core,
        )

    def channel_wait(d, step):
        return to_tp(
            channel.at[d], (channel_right if step > 0 else channel_left).at[d], c_send.at[d],
            (c_right if step > 0 else c_left).at[d], twin,
        )

    def project_twin(d):
        project(d, 1 - core, mix_twin)
        twin_mix(d).start()

    project_twin(order[0])
    for i, d in enumerate(order[:-1]):
        project_twin(order[i + 1])
        project(d, core, mix_own)
        take_row(arrival[i])
        mix_lead(d)
    project(chip, core, mix_own)

    for load in loads[5:]:
        load.wait()

    def twin_arrived(q):
        return to_tp(arrived.at[q, 0], arrived.at[q, 1], ta_send.at[q], ta_recv.at[q], twin)

    def twin_result(q):
        return to_tp(
            result_twin.at[q], result_in.at[q], ty_send.at[q], ty_recv.at[q], twin
        )

    def twin_shared(q):
        return to_tp(
            shared_twin.at[q], shared_in.at[q], th_send.at[q], th_recv.at[q], twin
        )

    def return_copy(q, k):
        target = flip(ep_index, k)
        return to_ep(
            result.at[q, target], returned.at[q, ep_index], r_send.at[q, k], r_recv.at[q, k],
            target,
        )

    def hand_over(q):
        for k in range(1, ep_count):
            dispatch_copy(q, k).wait_recv()
        twin_arrived(q).start()

    def gated_rows(rows, gate_weight, up_weight):
        gate_part = jnp.dot(rows, gate_weight, preferred_element_type=f32)
        up_part = jnp.dot(rows, up_weight, preferred_element_type=f32)
        return (gate_part / (1.0 + jnp.exp(-gate_part)) * up_part).astype(bf16)

    def shared(q):
        twin_row(q).wait_recv()
        rows = gathered[q, :, :, :width].reshape(CORES * tokens_here, width)
        hidden = gated_rows(rows, sg[...], su[...])
        product = jnp.dot(hidden, sd[...], preferred_element_type=f32).astype(bf16)
        shared_own[q] = product[:tokens_here]
        shared_twin[q] = product[tokens_here:]
        twin_shared(q).start()

    def experts(q):
        twin_arrived(q).wait_recv()
        for j in range(local_experts):
            cut = slice(j * capacity, (j + 1) * capacity)
            rows = arrived[q, :, :, cut, :].reshape(CORES * ep_count * capacity, width)
            hidden = gated_rows(rows, eg[j], eu[j])
            product = jnp.dot(hidden, ed[j], preferred_element_type=f32).astype(bf16)
            product = product.reshape(CORES, ep_count, capacity, width)
            result[q, :, cut, :] = product[0]
            result_twin[q, :, cut, :] = product[1]
        twin_result(q).start()

    def give_back(q):
        twin_result(q).wait_recv()
        result[q] = (result[q].astype(f32) + result_in[q].astype(f32)).astype(bf16)
        for k in range(1, ep_count):
            return_copy(q, k).start()
        returned[q, ep_index] = result[q, ep_index]

    hand_over(chip)
    shared(chip)
    experts(chip)
    mix_follow(order[0])
    for i, q in enumerate(order[:-1]):
        hand_over(q)
        shared(q)
        give_back(chip if i == 0 else order[i - 1])
        experts(q)
    for d in order[1:-1]:
        mix_follow(d)
    give_back(order[-2])

    def combined(q):
        for k in range(1, ep_count):
            return_copy(q, k).wait_recv()
        twin_shared(q).wait_recv()
        mixing = sum(
            jnp.where(
                slot_of(q, t) == slot_lane, weight_of(q, t), 0.0
            )
            for t in range(topk)
        )
        coarse = mixing.astype(bf16)
        fine = (mixing - coarse.astype(f32)).astype(bf16)
        rows = returned[q].reshape(slot_count, width)
        return (
            jnp.dot(coarse, rows, preferred_element_type=f32)
            + jnp.dot(fine, rows, preferred_element_type=f32)
            + shared_own[q].astype(f32)
            + shared_in[q].astype(f32)
        )

    def channel_on(d):
        own = combined(d)
        from_left = (chip > 0) & (d > chip)
        from_right = (chip < chips - 1) & (d < chip)

        @pl.when(from_left)
        def _():
            channel_wait(d, 1).wait_recv()
            channel[d] = (own + channel_right[d].astype(f32)).astype(bf16)

        @pl.when(from_right)
        def _():
            channel_wait(d, -1).wait_recv()
            channel[d] = (own + channel_left[d].astype(f32)).astype(bf16)

        @pl.when((chip == 0) | (chip == chips - 1))
        def _():
            channel[d] = own.astype(bf16)

        @pl.when(d > chip)
        def _():
            channel_step(d, 1).start()

        @pl.when(d < chip)
        def _():
            channel_step(d, -1).start()

    for d in order[:-1]:
        channel_on(d)

    def line_end(own, right_step, left_step, right_buffer, left_buffer, out_ref):
        out_ref[...] = own.astype(out_ref.dtype)

        @pl.when((chip > 0) & (chip < chips - 1))
        def _():
            right_step.wait_recv()
            left_step.wait_recv()
            out_ref[...] = (
                own + right_buffer[chip].astype(f32) + left_buffer[chip].astype(f32)
            ).astype(out_ref.dtype)

        @pl.when(chip == chips - 1)
        def _():
            right_step.wait_recv()
            out_ref[...] = (own + right_buffer[chip].astype(f32)).astype(out_ref.dtype)

        @pl.when(chip == 0)
        def _():
            left_step.wait_recv()
            out_ref[...] = (own + left_buffer[chip].astype(f32)).astype(out_ref.dtype)

    twin_mix(chip).wait_recv()
    line_end(
        mix_own[chip].astype(f32) + mix_in[chip].astype(f32), mix_wait(chip, 1),
        mix_wait(chip, -1), mix_right, mix_left, mixer_ref,
    )
    line_end(
        combined(chip), channel_wait(chip, 1), channel_wait(chip, -1), channel_right,
        channel_left, channel_out_ref,
    )

    for d in order[:-1]:
        @pl.when(reached(d))
        def _():
            gather_row(chip, d).wait_send()

        relay(d, lambda copy: copy.wait_send())
        mix_wait(d, 1).wait_send()
        channel_wait(d, 1).wait_send()
    for q in range(chips):
        twin_row(q).wait_send()
        twin_mix(q).wait_send()
        twin_arrived(q).wait_send()
        twin_result(q).wait_send()
        twin_shared(q).wait_send()
        for k in range(1, ep_count):
            dispatch_copy(q, k).wait_send()
            return_copy(q, k).wait_send()
    for k in range(1, ep_count):
        @pl.when(flip(ep_index, k) > ep_index)
        def _():
            total_copy(k).wait_send()
            for h in range(heads):
                state_copy(k, h).wait_send()


def turn_tables(key_width, sequence):
    half = key_width // 2
    inverse = np.float32(turn_base) ** (-np.arange(half, dtype=np.float32) / np.float32(half))
    inverse = inverse.astype(np.float64)

    def both(positions):
        angles = positions[:, None].astype(np.float64) * inverse[None, :]
        cosine, sine = np.cos(angles), np.sin(angles)
        return np.stack(
            [np.concatenate([cosine, cosine], axis=1), np.concatenate([-sine, sine], axis=1)]
        ).astype(np.float32)

    near = both(np.arange(BLOCK))
    far = both(np.arange(sequence // BLOCK) * BLOCK).transpose(1, 0, 2)
    return near, far


def whole_scratch(args, ep_count, chips, capacity):
    (
        query_rows, key_rows, value_rows, gate_rows, log_decay, out_weight, channel_input,
        _, _, _, expert_gate, expert_up, expert_down, shared_gate, shared_up, shared_down,
    ) = args
    f32, bf16 = jnp.float32, jnp.bfloat16
    tokens_here, width = channel_input.shape
    tokens, heads = query_rows.shape[0], log_decay.shape[0]
    key_width = query_rows.shape[1] // heads
    value_width = value_rows.shape[1] // heads
    blocks = tokens // BLOCK
    block_rows = expert_gate.shape[0] * capacity
    mixer_count = tokens // (chips * CORES)
    routed = (chips, ep_count, block_rows, width)
    rows = (chips, tokens_here, width)
    mixed = (chips, mixer_count, width)
    small = (8, 128)
    buffers = [(a.shape, a.dtype) for a in (
        query_rows, key_rows, value_rows, gate_rows, out_weight, expert_gate, expert_up,
        expert_down, shared_gate, shared_up, shared_down,
    )]
    buffers += [
        ((chips, CORES, tokens_here, width + 128), bf16),
        (routed, bf16), ((chips, CORES) + routed[1:], bf16), (routed, bf16), (routed, bf16),
        (routed, bf16), (routed, bf16),
    ]
    buffers += [(rows, bf16)] * 6 + [(mixed, bf16)] * 5
    buffers += [
        (value_rows.shape, bf16), (value_rows.shape, f32), (key_rows.shape, bf16),
        ((blocks, heads, key_width, value_width), f32), ((heads, key_width, value_width), f32),
        ((heads, key_width, value_width), bf16),
        ((ep_count, heads, key_width, value_width), bf16), (small, f32),
        ((ep_count,) + small, f32), ((blocks,) + small, f32), ((blocks * heads, BLOCK), f32),
        ((blocks, 8, BLOCK), f32), ((blocks, BLOCK, 128), f32),
    ]
    one, two, by_ep, by_head = (chips,), (chips, ep_count), (ep_count,), (ep_count, heads)
    counts = [(11,)] + [one] * 5 + [two] * 2 + [one] * 6 + [two] * 2 + [by_head] * 2 + [by_ep] * 2
    counts += [one] * 8
    return buffers, counts


def whole_step(args, ep_count, chips, capacity):
    (
        query_rows, key_rows, value_rows, gate_rows, log_decay, out_weight, channel_input,
        norm_gain, routes, route_weight, expert_gate, expert_up, expert_down, shared_gate,
        shared_up, shared_down,
    ) = args
    tokens_here, width = channel_input.shape
    tokens, heads = query_rows.shape[0], log_decay.shape[0]
    mixer_count = tokens // (chips * CORES)
    near, far = turn_tables(query_rows.shape[1] // heads, tokens * ep_count)
    buffers, counts = whole_scratch(args, ep_count, chips, capacity)
    vmem = pl.BlockSpec(memory_space=pltpu.VMEM)
    hbm = pl.BlockSpec(memory_space=pl.ANY)
    return pl.pallas_call(
        functools.partial(whole_kernel, (ep_count, chips, capacity)),
        out_shape=(
            jax.ShapeDtypeStruct((mixer_count, width), jnp.bfloat16),
            jax.ShapeDtypeStruct((tokens_here, width), jnp.bfloat16),
        ),
        in_specs=[vmem] * 7 + [hbm] * 11,
        out_specs=(vmem, vmem),
        scratch_shapes=[pltpu.VMEM(shape, dtype) for shape, dtype in buffers]
        + [pltpu.SemaphoreType.DMA(count) for count in counts],
        compiler_params=pltpu.CompilerParams(
            collective_id=0, has_side_effects=True, vmem_limit_bytes=KERNEL_VMEM
        ),
    )(
        channel_input, norm_gain.reshape(1, width), routes.T, route_weight.T, log_decay,
        jnp.asarray(near), jnp.asarray(far), query_rows, key_rows, value_rows, gate_rows,
        out_weight, expert_gate, expert_up, expert_down, shared_gate, shared_up, shared_down,
    )


def padded_bytes(shape, dtype):
    size = jnp.dtype(dtype).itemsize
    rows = 32 // size
    last = -(-shape[-1] // 128) * 128
    return math.prod(shape[:-2]) * (-(-shape[-2] // rows) * rows) * last * size


def one_kernel_fits(args, ep_count, chips, capacity):
    query_rows, log_decay, experts = args[0], args[4], args[10].shape[0] * ep_count
    heads = log_decay.shape[0]
    buffers, _ = whole_scratch(args, ep_count, chips, capacity)
    need = sum(padded_bytes(shape, dtype) for shape, dtype in buffers)
    return (
        chips > 1
        and capacity % 16 == 0
        and experts <= 128
        and experts * capacity <= 256
        and heads <= 8
        and query_rows.shape[1] // heads == 128
        and args[6].shape[0] % 16 == 0
        and need <= KERNEL_VMEM - (10 << 20)
    )


def local(
    query_rows, key_rows, value_rows, gate_rows, log_decay, out_weight, channel_input, norm_gain,
    routes, route_weight, expert_gate, expert_up, expert_down, shared_gate, shared_up, shared_down,
):
    ep_count, tp_count = lax.axis_size("ep"), lax.axis_size("tp")
    ep_index, tp_index = lax.axis_index("ep"), lax.axis_index("tp")
    chips = tp_count // CORES
    chip, core = tp_index // CORES, tp_index % CORES
    tokens_here, width = channel_input.shape
    topk = routes.shape[1]
    local_experts = expert_gate.shape[0]
    experts_all = ep_count * local_experts
    capacity = tokens_here * topk // experts_all + max(
        2, tokens_here * topk // (3 * experts_all)
    )

    args = (
        query_rows, key_rows, value_rows, gate_rows, log_decay, out_weight, channel_input,
        norm_gain, routes, route_weight, expert_gate, expert_up, expert_down, shared_gate,
        shared_up, shared_down,
    )
    if one_kernel_fits(args, ep_count, chips, capacity):
        return whole_step(args, ep_count, chips, capacity)

    wide = channel_input.astype(jnp.float32)
    normed = (
        wide * lax.rsqrt(jnp.mean(wide * wide, axis=-1, keepdims=True) + epsilon) * norm_gain
    ).astype(jnp.bfloat16)
    flat = routes.reshape(-1)
    onehot = (flat[:, None] == jnp.arange(experts_all, dtype=jnp.int32)[None, :]).astype(
        jnp.float32
    )
    count = tokens_here * topk
    before = (jnp.arange(count)[:, None] > jnp.arange(count)[None, :]).astype(jnp.float32)
    rank = jnp.sum(jnp.dot(before, onehot) * onehot, axis=1)
    notes = jnp.concatenate(
        [routes.astype(jnp.float32), rank.reshape(tokens_here, topk), route_weight], axis=1
    )
    notes = jnp.pad(notes, ((0, 0), (0, 128 - 3 * topk)))
    own_rows = line_gather(normed, chips)
    notes_all = line_gather(notes, chips)
    log_decay, normed, notes = lax.optimization_barrier((log_decay, normed, notes))
    route_all = notes_all[:, :, :topk].astype(jnp.int32)
    rank_all = notes_all[:, :, topk : 2 * topk].astype(jnp.int32)
    weight_all = notes_all[:, :, 2 * topk : 3 * topk]
    place = jnp.arange(chips, dtype=jnp.int32)[:, None, None]
    turn = (route_all // local_experts) ^ ep_index
    slot = ((turn * local_experts + route_all % local_experts) * chips + place) * capacity
    slot = (slot + rank_all).reshape(chips * tokens_here, topk)
    slot_count = experts_all * chips * capacity
    slot_ids = jnp.arange(slot_count, dtype=jnp.int32)
    placing = sum(
        (slot_ids[:, None] == slot[None, :, t]).astype(jnp.bfloat16) for t in range(topk)
    )
    own_flat = own_rows.reshape(chips * tokens_here, width)
    outgoing = jnp.dot(placing, own_flat, preferred_element_type=jnp.float32).astype(jnp.bfloat16)
    outgoing = outgoing.reshape(ep_count, local_experts, chips * capacity, width)
    arrived = [outgoing[0]] + [swap_ep(outgoing[k], k, ep_count) for k in range(1, ep_count)]
    own_twin = swap_cores(own_flat, tp_count)

    gated = retention(query_rows, key_rows, value_rows, gate_rows, log_decay)
    mixer_count = query_rows.shape[0] // tp_count
    gated_parts = gated.reshape(chips, CORES, mixer_count, gated.shape[1])

    def mixer_for(which):
        mine = lax.dynamic_index_in_dim(gated_parts, which, 1, keepdims=False)
        product = jnp.dot(
            mine.reshape(chips * mixer_count, -1), out_weight, preferred_element_type=jnp.float32
        )
        return product.astype(jnp.bfloat16)

    mixer_twin, mixer_mine = mixer_for(1 - core), mixer_for(core)
    mixer_half = summed(mixer_mine, swap_cores(mixer_twin, tp_count))
    arrived, _ = lax.optimization_barrier((arrived, (mixer_twin, mixer_mine)))
    arrived_twin = [swap_cores(block, tp_count) for block in arrived]
    mixer_half = mixer_half.reshape(chips, mixer_count, width)
    mixer_out = line_scatter(
        lambda r: lax.dynamic_index_in_dim(mixer_half, (chip + r) % chips, 0, False), chips
    ).astype(jnp.bfloat16)

    def experts_on(blocks, rows):
        routed = jnp.concatenate(blocks, axis=1)
        gate_part = jnp.einsum("emd,edf->emf", routed, expert_gate, preferred_element_type=jnp.float32)
        up_part = jnp.einsum("emd,edf->emf", routed, expert_up, preferred_element_type=jnp.float32)
        hidden = gated_pair(gate_part, up_part)
        routed_term = jnp.einsum(
            "emf,efd->emd", hidden, expert_down, preferred_element_type=jnp.float32
        ).astype(jnp.bfloat16)
        shared_hidden = gated_pair(
            jnp.dot(rows, shared_gate, preferred_element_type=jnp.float32),
            jnp.dot(rows, shared_up, preferred_element_type=jnp.float32),
        )
        shared_term = jnp.dot(
            shared_hidden, shared_down, preferred_element_type=jnp.float32
        ).astype(jnp.bfloat16)
        return routed_term, shared_term

    routed_twin, shared_twin = experts_on(arrived_twin, own_twin)
    routed_mine, shared_mine = experts_on(arrived, own_flat)
    routed = summed(routed_mine, swap_cores(routed_twin, tp_count))
    shared = summed(shared_mine, swap_cores(shared_twin, tp_count))
    routed = routed.reshape(local_experts, ep_count, chips * capacity, width)
    returned = [routed[:, 0]] + [swap_ep(routed[:, k], k, ep_count) for k in range(1, ep_count)]
    returned = jnp.stack(returned).reshape(slot_count, width)
    flat_weight = weight_all.reshape(chips * tokens_here, topk)
    mixing = sum(
        jnp.where(slot_ids[None, :] == slot[:, t : t + 1], flat_weight[:, t : t + 1], 0.0)
        for t in range(topk)
    )
    coarse = lax.reduce_precision(mixing, 8, 7)
    fine = (mixing - coarse).astype(jnp.bfloat16)
    coarse = coarse.astype(jnp.bfloat16)
    channel = (
        jnp.dot(coarse, returned, preferred_element_type=jnp.float32)
        + jnp.dot(fine, returned, preferred_element_type=jnp.float32)
        + shared.astype(jnp.float32)
    ).astype(jnp.bfloat16)
    channel = channel.reshape(chips, tokens_here, width)
    channel_out = line_scatter(lambda r: channel[(chips - r) % chips], chips).astype(jnp.bfloat16)
    return (mixer_out, channel_out)


def solution(mesh):
    in_specs = (
        P("ep", "tp"),
        P("ep", "tp"),
        P("ep", "tp"),
        P("ep", "tp"),
        P("tp", "ep"),
        P("tp", None),
        P(("ep", "tp"), None),
        P(),
        P(("ep", "tp"), None),
        P(("ep", "tp"), None),
        P("ep", None, "tp"),
        P("ep", None, "tp"),
        P("ep", "tp", None),
        P(None, "tp"),
        P(None, "tp"),
        P("tp", None),
    )
    out_specs = (P(("ep", "tp"), None), P(("ep", "tp"), None))
    return jax.shard_map(local, mesh=mesh, in_specs=in_specs, out_specs=out_specs, check_vma=False)
```

```python
import functools
import math

import jax
import jax.numpy as jnp
import numpy as np
from jax import lax
from jax.experimental import pallas as pl
from jax.experimental.pallas import tpu as pltpu
from jax.sharding import PartitionSpec as P

BLOCK = 128
CORES = 2
KERNEL_VMEM = 67043328

epsilon = 1e-06
turn_base = 10000.0


def shift_chips(array, r, count):
    pairs = [
        (z * CORES + c, (z + r) % count * CORES + c) for z in range(count) for c in range(CORES)
    ]
    return lax.ppermute(array, "tp", pairs)


def line_gather(array, count):
    return jnp.stack([array] + [shift_chips(array, r, count) for r in range(1, count)])


def line_scatter(part, count):
    total = part(0).astype(jnp.float32)
    for r in range(1, count):
        total = total + shift_chips(part(r), r, count).astype(jnp.float32)
    return total


def swap_cores(array, tp_count):
    return lax.ppermute(array, "tp", [(i, i ^ 1) for i in range(tp_count)])


def swap_ep(array, k, ep_count):
    return lax.ppermute(array, "ep", [(i, i ^ k) for i in range(ep_count)])


def turned(rows, cosine, sine):
    wide = rows.astype(jnp.float32)
    return (wide * cosine + pltpu.roll(wide, wide.shape[1] // 2, 1) * sine).astype(jnp.bfloat16)


def state_kernel(key_ref, value_ref, cosine_ref, sine_ref, fade_ref, state_ref):
    heads, key_width, value_width = state_ref.shape
    for h in range(heads):
        keys = turned(
            key_ref[:, h * key_width : (h + 1) * key_width], cosine_ref[...], sine_ref[...]
        )
        faded = (keys.astype(jnp.float32) * fade_ref[:, h : h + 1]).astype(jnp.bfloat16)
        state_ref[h] = lax.dot_general(
            faded,
            value_ref[:, h * value_width : (h + 1) * value_width],
            (((0,), (0,)), ((), ())),
            preferred_element_type=jnp.float32,
        ).astype(state_ref.dtype)


def retention_kernel(
    query_ref, key_ref, value_ref, gate_ref, cosine_ref, sine_ref, column_ref, row_ref,
    entry_ref, out_ref, state,
):
    heads, key_width, value_width = state.shape

    @pl.when(pl.program_id(0) == 0)
    def _():
        state[...] = entry_ref[...]

    cosine, sine = cosine_ref[...], sine_ref[...]
    lower = lax.broadcasted_iota(jnp.int32, (BLOCK, BLOCK), 0) >= lax.broadcasted_iota(
        jnp.int32, (BLOCK, BLOCK), 1
    )
    for h in range(heads):
        key_cut = slice(h * key_width, (h + 1) * key_width)
        value_cut = slice(h * value_width, (h + 1) * value_width)
        queries = turned(query_ref[:, key_cut], cosine, sine)
        keys = turned(key_ref[:, key_cut], cosine, sine)
        values = value_ref[:, value_cut]
        column = column_ref[:, h : h + 1]
        row = row_ref[0, h : h + 1, :]
        end = column_ref[BLOCK - 1 : BLOCK, h : h + 1]
        scores = lax.dot_general(
            queries, keys, (((1,), (1,)), ((), ())), preferred_element_type=jnp.float32
        )
        spread = jnp.exp(jnp.where(lower, column - row, 0.0))
        weights = jnp.where(lower, scores * spread, 0.0).astype(jnp.bfloat16)
        before = state[h]
        retained = jnp.dot(weights, values, preferred_element_type=jnp.float32)
        retained = retained + jnp.exp(column) * jnp.dot(
            queries, before.astype(jnp.bfloat16), preferred_element_type=jnp.float32
        )
        faded = (keys.astype(jnp.float32) * jnp.exp(end - column)).astype(jnp.bfloat16)
        state[h] = jnp.exp(end) * before + lax.dot_general(
            faded, values, (((0,), (0,)), ((), ())), preferred_element_type=jnp.float32
        )
        scale = lax.rsqrt(jnp.mean(retained * retained, axis=1, keepdims=True) + epsilon)
        gate = gate_ref[:, value_cut].astype(jnp.float32)
        out_ref[:, value_cut] = (gate / (1.0 + jnp.exp(-gate)) * (retained * scale)).astype(
            jnp.bfloat16
        )


def retention(query_rows, key_rows, value_rows, gate_rows, log_decay):
    tokens = query_rows.shape[0]
    heads = log_decay.shape[0]
    key_width = query_rows.shape[1] // heads
    value_width = value_rows.shape[1] // heads
    blocks = tokens // BLOCK
    ep_count, ep_index = lax.axis_size("ep"), lax.axis_index("ep")
    half = key_width // 2
    position = (ep_index * tokens + jnp.arange(tokens, dtype=jnp.int32)).astype(jnp.float32)
    inverse = turn_base ** (-jnp.arange(half, dtype=jnp.float32) / half)
    angles = position[:, None] * inverse[None, :]
    cosine, sine = jnp.cos(angles), jnp.sin(angles)
    cosine = jnp.concatenate([cosine, cosine], axis=1)
    sine = jnp.concatenate([-sine, sine], axis=1)
    running = jnp.cumsum(log_decay.reshape(heads, blocks, BLOCK), axis=2)
    ends = running[:, :, -1]
    later = jnp.sum(ends, axis=1, keepdims=True) - jnp.cumsum(ends, axis=1)
    later = jnp.minimum(later, 0.0)
    fade = jnp.exp(ends[:, :, None] - running + later[:, :, None]).reshape(heads, tokens).T
    total = jnp.sum(ends, axis=1)
    vmem = pl.BlockSpec(memory_space=pltpu.VMEM)
    own_state = pl.pallas_call(
        state_kernel,
        out_shape=jax.ShapeDtypeStruct((heads, key_width, value_width), jnp.bfloat16),
        in_specs=[vmem] * 5,
        out_specs=vmem,
        cost_estimate=pl.CostEstimate(
            flops=2 * tokens * heads * key_width * value_width * 4,
            bytes_accessed=8 << 20,
            transcendentals=0,
        ),
    )(key_rows, value_rows, cosine, sine, fade)
    totals_sent = jnp.broadcast_to(total[:, None], (heads, 128))
    states, totals = [], [total]
    for k in range(1, ep_count):
        states.append(swap_ep(own_state, k, ep_count))
        totals.append(swap_ep(totals_sent, k, ep_count)[:, 0])
    entry = jnp.zeros((heads, key_width, value_width), jnp.float32)
    for k in range(1, ep_count):
        source = ep_index ^ k
        passed = jnp.zeros_like(total)
        for m in range(1, ep_count):
            between = ((ep_index ^ m) > source) & ((ep_index ^ m) < ep_index)
            passed = passed + jnp.where(between, totals[m], 0.0)
        share = jnp.where(source < ep_index, jnp.exp(passed), 0.0)
        entry = entry + share[:, None, None] * states[k - 1].astype(jnp.float32)
    columns = running.reshape(heads, tokens).T
    rows = running.transpose(1, 0, 2)
    by_block = lambda width: pl.BlockSpec((BLOCK, width), lambda n: (n, 0))
    whole = pl.BlockSpec((heads, key_width, value_width), lambda n: (0, 0, 0))
    return pl.pallas_call(
        retention_kernel,
        out_shape=jax.ShapeDtypeStruct((tokens, heads * value_width), jnp.bfloat16),
        grid=(blocks,),
        in_specs=[
            by_block(heads * key_width),
            by_block(heads * key_width),
            by_block(heads * value_width),
            by_block(heads * value_width),
            by_block(key_width),
            by_block(key_width),
            by_block(heads),
            pl.BlockSpec((1, heads, BLOCK), lambda n: (n, 0, 0)),
            whole,
        ],
        out_specs=by_block(heads * value_width),
        scratch_shapes=[pltpu.VMEM((heads, key_width, value_width), jnp.float32)],
        cost_estimate=pl.CostEstimate(
            flops=8 << 30, bytes_accessed=24 << 20, transcendentals=0
        ),
    )(query_rows, key_rows, value_rows, gate_rows, cosine, sine, columns, rows, entry)


def gated_pair(gate_part, up_part):
    return (jax.nn.silu(gate_part) * up_part).astype(jnp.bfloat16)


def summed(a, b):
    return (a.astype(jnp.float32) + b.astype(jnp.float32)).astype(jnp.bfloat16)


def flip(index, k):
    turned_index, bit = index, 1
    while bit <= k:
        if k & bit:
            turned_index = turned_index + bit - 2 * bit * ((index // bit) % 2)
        bit *= 2
    return turned_index


def line_order(chips):
    orders = []
    for z in range(chips):
        right, left = list(range(chips - 1, z, -1)), list(range(z))
        order = []
        sides = [right, left] if len(right) >= len(left) else [left, right]
        while right or left:
            if sides[0]:
                order.append(sides[0].pop(0))
            sides.reverse()
        orders.append(order + [z])
    return orders


def arrival_order(chips):
    def rank(z, q):
        hands_on = (q <= z - 2 and z < chips - 1) or (q >= z + 2 and z > 0)
        return (not hands_on, abs(q - z), q)

    return [
        sorted((q for q in range(chips) if q != z), key=functools.partial(rank, z))
        for z in range(chips)
    ]


def pick(table, index):
    chosen = 0
    for i, entry in enumerate(table):
        chosen = chosen + jnp.where(index == i, entry, 0)
    return chosen


def in_steps(count, together, body):
    together = math.gcd(count, together)

    def step(i, carry):
        for j in range(together):
            body(i * together + j)
        return carry

    lax.fori_loop(0, count // together, step, 0)


def whole_kernel(
    sizes,
    channel_ref, gain_ref, routes_ref, weight_ref, decay_ref, near_ref, far_ref,
    query_any, key_any, value_any, gate_any, out_any, eg_any, eu_any, ed_any, sg_any, su_any,
    sd_any,
    mixer_ref, channel_out_ref,
    query, key, value, gate, out_w, eg, eu, ed, sg, su, sd,
    gathered, slots, arrived, result_twin, result_in, result, returned,
    shared_twin, shared_in, shared_own, channel, channel_right, channel_left,
    mix_twin, mix_in, mix_own, mix_right, mix_left,
    gated, partial, keys_turned, before, entry, state_send, state_in, total_send, total_in, prefix,
    decay_flat, run_row, run_col,
    local_sem, g_send, g_recv, f_send, tg_send, tg_recv, d_send, d_recv, ta_send, ta_recv,
    ty_send, ty_recv, th_send, th_recv, r_send, r_recv, s_send, s_recv, o_send, o_recv,
    tp_send, tp_recv, m_send, m_right, m_left, c_send, c_right, c_left,
):
    ep_count, chips, capacity = sizes
    f32, bf16 = jnp.float32, jnp.bfloat16
    tokens_here, width = channel_ref.shape
    topk = routes_ref.shape[0]
    local_experts = eg.shape[0]
    block_rows = local_experts * capacity
    slot_count = ep_count * block_rows
    heads, key_width, value_width = entry.shape
    blocks = before.shape[0]
    mixer_count = mixer_ref.shape[0]
    ep_index, tp_index = lax.axis_index("ep"), lax.axis_index("tp")
    chip, core = tp_index // CORES, tp_index % CORES
    twin = tp_index + 1 - 2 * core
    orders = line_order(chips)
    order = [pick([row[i] for row in orders], chip) for i in range(chips - 1)] + [chip]
    arrivals = arrival_order(chips)
    arrival = [pick([row[i] for row in arrivals], chip) for i in range(chips - 1)]

    def to_tp(src, dst, send, recv, target):
        return pltpu.make_async_remote_copy(
            src_ref=src, dst_ref=dst, send_sem=send, recv_sem=recv,
            device_id={"tp": target}, device_id_type=pl.DeviceIdType.MESH,
        )

    def to_ep(src, dst, send, recv, target):
        return pltpu.make_async_remote_copy(
            src_ref=src, dst_ref=dst, send_sem=send, recv_sem=recv,
            device_id={"ep": target}, device_id_type=pl.DeviceIdType.MESH,
        )

    barrier = pltpu.get_barrier_semaphore()
    for r in range(1, chips):
        pl.semaphore_signal(
            barrier, inc=1, device_id={"tp": (chip + r) % chips * CORES + core},
            device_id_type=pl.DeviceIdType.MESH,
        )
    pl.semaphore_signal(
        barrier, inc=1, device_id={"tp": twin}, device_id_type=pl.DeviceIdType.MESH
    )
    for k in range(1, ep_count):
        pl.semaphore_signal(
            barrier, inc=1, device_id={"ep": flip(ep_index, k)},
            device_id_type=pl.DeviceIdType.MESH,
        )

    pairs = [
        (key_any, key), (value_any, value), (query_any, query), (gate_any, gate),
        (out_any, out_w), (sg_any, sg), (su_any, su), (sd_any, sd), (eg_any, eg), (eu_any, eu),
        (ed_any, ed),
    ]
    loads = [pltpu.make_async_copy(s, d, local_sem.at[i]) for i, (s, d) in enumerate(pairs)]
    for load in loads:
        load.start()

    wide = channel_ref[...].astype(f32)
    normed = (
        wide * lax.rsqrt(jnp.mean(wide * wide, axis=-1, keepdims=True) + epsilon) * gain_ref[...]
    ).astype(bf16)
    gathered[chip, 0, :, :width] = normed
    lane = lax.broadcasted_iota(jnp.int32, (tokens_here, 128), 1)
    same = (
        lax.broadcasted_iota(jnp.int32, (tokens_here, tokens_here), 0)
        == lax.broadcasted_iota(jnp.int32, (tokens_here, tokens_here), 1)
    ).astype(f32)

    def as_columns(rows):
        return lax.dot_general(
            same, rows, (((1,), (1,)), ((), ())), preferred_element_type=f32,
            precision=lax.Precision.HIGHEST,
        )

    route_columns = as_columns(routes_ref[...].astype(f32))
    weight_columns = as_columns(weight_ref[...])
    routed_to = [route_columns[:, t : t + 1] for t in range(topk)]
    named = [(route == lane.astype(f32)).astype(f32) for route in routed_to]
    earlier = (
        lax.broadcasted_iota(jnp.int32, (tokens_here, tokens_here), 0)
        > lax.broadcasted_iota(jnp.int32, (tokens_here, tokens_here), 1)
    ).astype(bf16)
    ahead = jnp.dot(earlier, sum(named).astype(bf16), preferred_element_type=f32)
    noted = jnp.zeros((tokens_here, 128), f32)
    for t in range(topk):
        rank = jnp.sum(ahead * named[t], axis=1, keepdims=True)
        noted = jnp.where(lane == t, routed_to[t] * capacity + rank, noted)
        left = weight_columns[:, t : t + 1]
        for piece in range(3):
            term = left.astype(bf16).astype(f32)
            noted = jnp.where(lane == topk + 3 * t + piece, term, noted)
            left = left - term
    gathered[chip, 0, :, width:] = noted.astype(bf16)

    def slot_of(q, t):
        return gathered[q, 0, :, width:].astype(f32)[:, t : t + 1]

    def weight_of(q, t):
        terms = gathered[q, 0, :, width:].astype(f32)
        at = topk + 3 * t
        return terms[:, at : at + 1] + terms[:, at + 1 : at + 2] + terms[:, at + 2 : at + 3]

    pl.semaphore_wait(barrier, chips + ep_count - 1)

    def gather_row(q, target):
        return to_tp(
            gathered.at[q, 0], gathered.at[q, 0], g_send.at[target], g_recv.at[q],
            target * CORES + core,
        )

    def relay_row(q, target):
        return to_tp(
            gathered.at[q, 0], gathered.at[q, 0], f_send.at[q], g_recv.at[q],
            target * CORES + core,
        )

    def relay(q, act):
        @pl.when((q <= chip - 2) & (chip < chips - 1))
        def _():
            act(relay_row(q, chip + 1))

        @pl.when((q >= chip + 2) & (chip > 0))
        def _():
            act(relay_row(q, chip - 1))

    def twin_row(q):
        return to_tp(
            gathered.at[q, 0], gathered.at[q, 1], tg_send.at[q], tg_recv.at[q], twin
        )

    def reached(target):
        return (target - chip) * (target - chip) <= 4

    for target in order[:-1]:
        @pl.when(reached(target))
        def _():
            gather_row(chip, target).start()

    twin_row(chip).start()

    slot_lane = lax.broadcasted_iota(jnp.int32, (tokens_here, slot_count), 1).astype(f32)

    def dispatch_copy(q, k):
        target = flip(ep_index, k)
        return to_ep(
            slots.at[q, target], arrived.at[q, 0, ep_index], d_send.at[q, k], d_recv.at[q, k],
            target,
        )

    def dispatch(q):
        placing = sum(
            (slot_of(q, t) == slot_lane).astype(f32) for t in range(topk)
        ).astype(bf16)
        rows = lax.dot_general(
            placing, gathered[q, 0, :, :width], (((0,), (0,)), ((), ())), preferred_element_type=f32
        ).astype(bf16)
        slots[q] = rows.reshape(ep_count, block_rows, width)
        for k in range(1, ep_count):
            dispatch_copy(q, k).start()
        arrived[q, 0, ep_index] = slots[q, ep_index]

    def take_row(q):
        gather_row(q, q).wait_recv()
        relay(q, lambda copy: copy.start())
        twin_row(q).start()
        dispatch(q)

    for n in range(blocks):
        decay_flat[n * heads : (n + 1) * heads, :] = decay_ref[:, n * BLOCK : (n + 1) * BLOCK]
    upper = (
        lax.broadcasted_iota(jnp.int32, (BLOCK, BLOCK), 0)
        <= lax.broadcasted_iota(jnp.int32, (BLOCK, BLOCK), 1)
    )
    lower = (
        lax.broadcasted_iota(jnp.int32, (BLOCK, BLOCK), 0)
        >= lax.broadcasted_iota(jnp.int32, (BLOCK, BLOCK), 1)
    )
    flat = decay_flat[...]
    by_row = jnp.dot(
        flat, upper.astype(f32), preferred_element_type=f32, precision=lax.Precision.HIGHEST
    )
    by_col = lax.dot_general(
        lower.astype(f32), flat, (((1,), (1,)), ((), ())), preferred_element_type=f32,
        precision=lax.Precision.HIGHEST,
    )
    for n in range(blocks):
        run_row[n] = jnp.zeros(run_row.shape[1:], f32)
        run_row[n, 0:heads, :] = by_row[n * heads : (n + 1) * heads, :]
        run_col[n, :, 0:heads] = by_col[:, n * heads : (n + 1) * heads]

    def turns(n):
        far = far_ref[ep_index * blocks + n]
        far_cos, far_sin = far[0:1, :], far[1:2, :]
        near_cos, near_sin = near_ref[0], near_ref[1]
        return near_cos * far_cos - near_sin * far_sin, near_sin * far_cos + near_cos * far_sin

    whole_decay = jnp.zeros(total_send.shape, f32)
    for n in range(blocks):
        prefix[n] = whole_decay
        whole_decay = whole_decay + run_row[n, :, BLOCK - 1 : BLOCK]
    total_send[...] = whole_decay

    def state_copy(k, h):
        return to_ep(
            state_send.at[h], state_in.at[k, h], s_send.at[k, h], s_recv.at[k, h],
            flip(ep_index, k),
        )

    def total_copy(k):
        return to_ep(
            total_send, total_in.at[k], o_send.at[k], o_recv.at[k], flip(ep_index, k)
        )

    for k in range(1, ep_count):
        @pl.when(flip(ep_index, k) > ep_index)
        def _():
            total_copy(k).start()

    loads[0].wait()
    loads[1].wait()

    def first_pass(h):
        key_cut = slice(h * key_width, (h + 1) * key_width)
        value_cut = slice(h * value_width, (h + 1) * value_width)
        held = jnp.zeros((key_width, value_width), f32)
        for n in range(blocks):
            at = slice(n * BLOCK, (n + 1) * BLOCK)
            keys = turned(key[at, key_cut], *turns(n))
            keys_turned[at, key_cut] = keys
            end = run_row[n, h : h + 1, BLOCK - 1 : BLOCK]
            faded = (keys.astype(f32) * jnp.exp(end - run_col[n, :, h : h + 1])).astype(bf16)
            before[n, h] = held
            held = jnp.exp(end) * held + lax.dot_general(
                faded, value[at, value_cut], (((0,), (0,)), ((), ())),
                preferred_element_type=f32,
            )
        state_send[h] = held.astype(bf16)

    for h in range(heads):
        first_pass(h)
        for k in range(1, ep_count):
            @pl.when(flip(ep_index, k) > ep_index)
            def _():
                state_copy(k, h).start()

    loads[2].wait()

    def second_pass(n):
        at = pl.ds(pl.multiple_of(n * BLOCK, BLOCK), BLOCK)
        cosine, sine = turns(n)
        for h in range(heads):
            key_cut = slice(h * key_width, (h + 1) * key_width)
            value_cut = slice(h * value_width, (h + 1) * value_width)
            queries = turned(query[at, key_cut], cosine, sine)
            query[at, key_cut] = queries
            column = run_col[n, :, h : h + 1]
            row = run_row[n, h : h + 1, :]
            scores = lax.dot_general(
                queries, keys_turned[at, key_cut], (((1,), (1,)), ((), ())),
                preferred_element_type=f32,
            )
            spread = jnp.exp(jnp.where(lower, column - row, 0.0))
            weights = jnp.where(lower, scores * spread, 0.0).astype(bf16)
            partial[at, value_cut] = jnp.dot(
                weights, value[at, value_cut], preferred_element_type=f32
            ) + jnp.exp(column) * jnp.dot(
                queries, before[n, h].astype(bf16), preferred_element_type=f32
            )

    in_steps(blocks, 2, second_pass)
    take_row(arrival[0])

    loads[3].wait()
    for k in range(1, ep_count):
        @pl.when(flip(ep_index, k) < ep_index)
        def _():
            total_copy(k).wait_recv()

        @pl.when(flip(ep_index, k) > ep_index)
        def _():
            total_in[k] = jnp.zeros_like(total_send)
            state_in[k] = jnp.zeros_like(state_send)

    shares = []
    for k in range(1, ep_count):
        source = flip(ep_index, k)
        passed = jnp.zeros(total_send.shape, f32)
        for m in range(1, ep_count):
            between = (flip(ep_index, m) > source) & (flip(ep_index, m) < ep_index)
            passed = passed + jnp.where(between, total_in[m], 0.0)
        shares.append(jnp.where(source < ep_index, jnp.exp(passed), 0.0))

    def third_pass(h):
        for k in range(1, ep_count):
            @pl.when(flip(ep_index, k) < ep_index)
            def _():
                state_copy(k, h).wait_recv()

        entry[h] = sum(
            shares[k - 1][h : h + 1, 0:1] * state_in[k, h].astype(f32)
            for k in range(1, ep_count)
        )
        value_cut = slice(h * value_width, (h + 1) * value_width)

        def finish(n):
            at = pl.ds(pl.multiple_of(n * BLOCK, BLOCK), BLOCK)
            grown = jnp.exp(run_col[n, :, h : h + 1] + prefix[n, h : h + 1, 0:1])
            retained = partial[at, value_cut] + grown * jnp.dot(
                query[at, h * key_width : (h + 1) * key_width], entry[h].astype(bf16),
                preferred_element_type=f32,
            )
            scale = lax.rsqrt(jnp.mean(retained * retained, axis=1, keepdims=True) + epsilon)
            gates = gate[at, value_cut].astype(f32)
            gated[at, value_cut] = (
                gates / (1.0 + jnp.exp(-gates)) * (retained * scale)
            ).astype(bf16)

        in_steps(blocks, 4, finish)

    for h in range(heads):
        third_pass(h)

    loads[4].wait()

    def twin_mix(d):
        return to_tp(mix_twin.at[d], mix_in.at[d], tp_send.at[d], tp_recv.at[d], twin)

    def project(d, which, into):
        start = pl.multiple_of((d * CORES + which) * mixer_count, mixer_count)
        into[d] = jnp.dot(
            gated[pl.ds(start, mixer_count), :], out_w[...], preferred_element_type=f32
        ).astype(bf16)

    def mix_copy(d, half, step, target):
        rows = pl.ds(half * (mixer_count // 2), mixer_count // 2)
        return to_tp(
            mix_own.at[d, rows], (mix_right if step > 0 else mix_left).at[d, rows],
            m_send.at[d, half], (m_right if step > 0 else m_left).at[d, half], target,
        )

    def mix_step(d, half, step):
        return mix_copy(d, half, step, (chip + step) * CORES + core)

    def mix_wait(d, half, step):
        return mix_copy(d, half, step, twin)

    def mix_sum(d, half, *others):
        rows = pl.ds(half * (mixer_count // 2), mixer_count // 2)
        total = mix_own[d, rows].astype(f32) + mix_in[d, rows].astype(f32)
        for other in others:
            total = total + other[d, rows].astype(f32)
        mix_own[d, rows] = total.astype(bf16)

    def mix_lead(d, halves):
        @pl.when((chip == 0) | (chip == chips - 1))
        def _():
            for half in halves:
                mix_sum(d, half)

        @pl.when(chip == 0)
        def _():
            for half in halves:
                mix_step(d, half, 1).start()

        @pl.when(chip == chips - 1)
        def _():
            for half in halves:
                mix_step(d, half, -1).start()

    def mix_follow(d, half):
        @pl.when((chip > 0) & (d > chip))
        def _():
            mix_wait(d, half, 1).wait_recv()
            mix_sum(d, half, mix_right)
            mix_step(d, half, 1).start()

        @pl.when((chip < chips - 1) & (d < chip))
        def _():
            mix_wait(d, half, -1).wait_recv()
            mix_sum(d, half, mix_left)
            mix_step(d, half, -1).start()

    def channel_step(d, step):
        return to_tp(
            channel.at[d], (channel_right if step > 0 else channel_left).at[d], c_send.at[d],
            (c_right if step > 0 else c_left).at[d], (chip + step) * CORES + core,
        )

    def channel_wait(d, step):
        return to_tp(
            channel.at[d], (channel_right if step > 0 else channel_left).at[d], c_send.at[d],
            (c_right if step > 0 else c_left).at[d], twin,
        )

    def project_twin(d):
        project(d, 1 - core, mix_twin)
        twin_mix(d).start()

    project_twin(order[0])
    rows_left = arrival[1:]
    for i, d in enumerate(order[:-1]):
        project_twin(order[i + 1])
        project(d, core, mix_own)
        twin_mix(d).wait_recv()
        mix_lead(d, (0, 1) if i + 2 < chips else (0,))
        for q in rows_left[:1] if i == 0 else rows_left if i + 2 == chips else ():
            take_row(q)
            rows_left = rows_left[1:]
    project(chip, core, mix_own)

    for load in loads[5:]:
        load.wait()

    def twin_arrived(q):
        return to_tp(arrived.at[q, 0], arrived.at[q, 1], ta_send.at[q], ta_recv.at[q], twin)

    def twin_result(q):
        return to_tp(
            result_twin.at[q], result_in.at[q], ty_send.at[q], ty_recv.at[q], twin
        )

    def twin_shared(q):
        return to_tp(
            shared_twin.at[q], shared_in.at[q], th_send.at[q], th_recv.at[q], twin
        )

    def return_copy(q, k):
        target = flip(ep_index, k)
        return to_ep(
            result.at[q, target], returned.at[q, ep_index], r_send.at[q, k], r_recv.at[q, k],
            target,
        )

    def hand_over(q):
        for k in range(1, ep_count):
            dispatch_copy(q, k).wait_recv()
        twin_arrived(q).start()

    def gated_rows(rows, gate_weight, up_weight):
        gate_part = jnp.dot(rows, gate_weight, preferred_element_type=f32)
        up_part = jnp.dot(rows, up_weight, preferred_element_type=f32)
        return (gate_part / (1.0 + jnp.exp(-gate_part)) * up_part).astype(bf16)

    def shared(q):
        twin_row(q).wait_recv()
        rows = gathered[q, :, :, :width].reshape(CORES * tokens_here, width)
        hidden = gated_rows(rows, sg[...], su[...])
        product = jnp.dot(hidden, sd[...], preferred_element_type=f32).astype(bf16)
        shared_own[q] = product[:tokens_here]
        shared_twin[q] = product[tokens_here:]
        twin_shared(q).start()

    def experts(q):
        twin_arrived(q).wait_recv()
        for j in range(local_experts):
            cut = slice(j * capacity, (j + 1) * capacity)
            rows = arrived[q, :, :, cut, :].reshape(CORES * ep_count * capacity, width)
            hidden = gated_rows(rows, eg[j], eu[j])
            product = jnp.dot(hidden, ed[j], preferred_element_type=f32).astype(bf16)
            product = product.reshape(CORES, ep_count, capacity, width)
            result[q, :, cut, :] = product[0]
            result_twin[q, :, cut, :] = product[1]
        twin_result(q).start()

    def give_back(q):
        twin_result(q).wait_recv()
        result[q] = (result[q].astype(f32) + result_in[q].astype(f32)).astype(bf16)
        for k in range(1, ep_count):
            return_copy(q, k).start()
        returned[q, ep_index] = result[q, ep_index]

    others = order[:-1]
    for q in arrival + [chip]:
        shared(q)
    dispatch(chip)
    for half in range(2):
        mix_follow(others[0], half)
    for q in others:
        hand_over(q)
    for i, q in enumerate(others):
        experts(q)
        if i > 0:
            give_back(others[i - 1])
    hand_over(chip)
    for d in others[1:]:
        mix_follow(d, 0)
    give_back(others[-1])
    experts(chip)
    for d in others[1:]:
        mix_follow(d, 1)
    give_back(chip)

    def combined(q):
        for k in range(1, ep_count):
            return_copy(q, k).wait_recv()
        twin_shared(q).wait_recv()
        mixing = sum(
            jnp.where(
                slot_of(q, t) == slot_lane, weight_of(q, t), 0.0
            )
            for t in range(topk)
        )
        coarse = mixing.astype(bf16)
        fine = (mixing - coarse.astype(f32)).astype(bf16)
        rows = returned[q].reshape(slot_count, width)
        return (
            jnp.dot(coarse, rows, preferred_element_type=f32)
            + jnp.dot(fine, rows, preferred_element_type=f32)
            + shared_own[q].astype(f32)
            + shared_in[q].astype(f32)
        )

    def channel_on(d):
        own = combined(d)
        from_left = (chip > 0) & (d > chip)
        from_right = (chip < chips - 1) & (d < chip)

        @pl.when(from_left)
        def _():
            channel_wait(d, 1).wait_recv()
            channel[d] = (own + channel_right[d].astype(f32)).astype(bf16)

        @pl.when(from_right)
        def _():
            channel_wait(d, -1).wait_recv()
            channel[d] = (own + channel_left[d].astype(f32)).astype(bf16)

        @pl.when((chip == 0) | (chip == chips - 1))
        def _():
            channel[d] = own.astype(bf16)

        @pl.when(d > chip)
        def _():
            channel_step(d, 1).start()

        @pl.when(d < chip)
        def _():
            channel_step(d, -1).start()

    for i, d in enumerate(order[:-1]):
        channel_on(d)
        if i == 0:
            mix_lead(order[-2], (1,))

    def line_end(own, right_waits, left_waits, right_buffer, left_buffer, into):
        into[chip] = own.astype(bf16)

        @pl.when(chip > 0)
        def _():
            for wait in right_waits:
                wait.wait_recv()

        @pl.when(chip < chips - 1)
        def _():
            for wait in left_waits:
                wait.wait_recv()

        @pl.when((chip > 0) & (chip < chips - 1))
        def _():
            into[chip] = (
                own + right_buffer[chip].astype(f32) + left_buffer[chip].astype(f32)
            ).astype(bf16)

        @pl.when(chip == chips - 1)
        def _():
            into[chip] = (own + right_buffer[chip].astype(f32)).astype(bf16)

        @pl.when(chip == 0)
        def _():
            into[chip] = (own + left_buffer[chip].astype(f32)).astype(bf16)

    twin_mix(chip).wait_recv()
    line_end(
        mix_own[chip].astype(f32) + mix_in[chip].astype(f32),
        [mix_wait(chip, half, 1) for half in range(2)],
        [mix_wait(chip, half, -1) for half in range(2)], mix_right, mix_left, mix_own,
    )
    mixer_store = pltpu.make_async_copy(mix_own.at[chip], mixer_ref, local_sem.at[len(pairs)])
    mixer_store.start()
    line_end(
        combined(chip), [channel_wait(chip, 1)], [channel_wait(chip, -1)], channel_right,
        channel_left, channel,
    )
    channel_store = pltpu.make_async_copy(
        channel.at[chip], channel_out_ref, local_sem.at[len(pairs) + 1]
    )
    channel_store.start()

    for d in order[:-1]:
        @pl.when(reached(d))
        def _():
            gather_row(chip, d).wait_send()

        relay(d, lambda copy: copy.wait_send())
        mix_wait(d, 0, 1).wait_send()
        mix_wait(d, 1, 1).wait_send()
        channel_wait(d, 1).wait_send()
    for q in range(chips):
        twin_row(q).wait_send()
        twin_mix(q).wait_send()
        twin_arrived(q).wait_send()
        twin_result(q).wait_send()
        twin_shared(q).wait_send()
        for k in range(1, ep_count):
            dispatch_copy(q, k).wait_send()
            return_copy(q, k).wait_send()
    for k in range(1, ep_count):
        @pl.when(flip(ep_index, k) > ep_index)
        def _():
            total_copy(k).wait_send()
            for h in range(heads):
                state_copy(k, h).wait_send()

    mixer_store.wait()
    channel_store.wait()


def turn_tables(key_width, sequence):
    half = key_width // 2
    inverse = np.float32(turn_base) ** (-np.arange(half, dtype=np.float32) / np.float32(half))
    inverse = inverse.astype(np.float64)

    def both(positions):
        angles = positions[:, None].astype(np.float64) * inverse[None, :]
        cosine, sine = np.cos(angles), np.sin(angles)
        return np.stack(
            [np.concatenate([cosine, cosine], axis=1), np.concatenate([-sine, sine], axis=1)]
        ).astype(np.float32)

    near = both(np.arange(BLOCK))
    far = both(np.arange(sequence // BLOCK) * BLOCK).transpose(1, 0, 2)
    return near, far


def whole_scratch(args, ep_count, chips, capacity):
    (
        query_rows, key_rows, value_rows, gate_rows, log_decay, out_weight, channel_input,
        _, _, _, expert_gate, expert_up, expert_down, shared_gate, shared_up, shared_down,
    ) = args
    f32, bf16 = jnp.float32, jnp.bfloat16
    tokens_here, width = channel_input.shape
    tokens, heads = query_rows.shape[0], log_decay.shape[0]
    key_width = query_rows.shape[1] // heads
    value_width = value_rows.shape[1] // heads
    blocks = tokens // BLOCK
    block_rows = expert_gate.shape[0] * capacity
    mixer_count = tokens // (chips * CORES)
    routed = (chips, ep_count, block_rows, width)
    rows = (chips, tokens_here, width)
    mixed = (chips, mixer_count, width)
    small = (8, 128)
    buffers = [(a.shape, a.dtype) for a in (
        query_rows, key_rows, value_rows, gate_rows, out_weight, expert_gate, expert_up,
        expert_down, shared_gate, shared_up, shared_down,
    )]
    buffers += [
        ((chips, CORES, tokens_here, width + 128), bf16),
        (routed, bf16), ((chips, CORES) + routed[1:], bf16), (routed, bf16), (routed, bf16),
        (routed, bf16), (routed, bf16),
    ]
    buffers += [(rows, bf16)] * 6 + [(mixed, bf16)] * 5
    buffers += [
        (value_rows.shape, bf16), (value_rows.shape, f32), (key_rows.shape, bf16),
        ((blocks, heads, key_width, value_width), f32), ((heads, key_width, value_width), f32),
        ((heads, key_width, value_width), bf16),
        ((ep_count, heads, key_width, value_width), bf16), (small, f32),
        ((ep_count,) + small, f32), ((blocks,) + small, f32), ((blocks * heads, BLOCK), f32),
        ((blocks, 8, BLOCK), f32), ((blocks, BLOCK, 128), f32),
    ]
    one, two, by_ep, by_head = (chips,), (chips, ep_count), (ep_count,), (ep_count, heads)
    counts = [(13,)] + [one] * 5 + [two] * 2 + [one] * 6 + [two] * 2 + [by_head] * 2 + [by_ep] * 2
    counts += [one] * 2 + [(chips, 2)] * 3 + [one] * 3
    return buffers, counts


def whole_step(args, ep_count, chips, capacity):
    (
        query_rows, key_rows, value_rows, gate_rows, log_decay, out_weight, channel_input,
        norm_gain, routes, route_weight, expert_gate, expert_up, expert_down, shared_gate,
        shared_up, shared_down,
    ) = args
    tokens_here, width = channel_input.shape
    tokens, heads = query_rows.shape[0], log_decay.shape[0]
    mixer_count = tokens // (chips * CORES)
    near, far = turn_tables(query_rows.shape[1] // heads, tokens * ep_count)
    buffers, counts = whole_scratch(args, ep_count, chips, capacity)
    vmem = pl.BlockSpec(memory_space=pltpu.VMEM)
    hbm = pl.BlockSpec(memory_space=pl.ANY)
    results = pl.pallas_call(
        functools.partial(whole_kernel, (ep_count, chips, capacity)),
        out_shape=(
            jax.ShapeDtypeStruct((mixer_count, width), jnp.bfloat16),
            jax.ShapeDtypeStruct((tokens_here, width), jnp.bfloat16),
        ),
        in_specs=[vmem] * 7 + [hbm] * 11,
        out_specs=(hbm, hbm),
        scratch_shapes=[pltpu.VMEM(shape, dtype) for shape, dtype in buffers]
        + [pltpu.SemaphoreType.DMA(count) for count in counts],
        compiler_params=pltpu.CompilerParams(
            collective_id=0, has_side_effects=True, vmem_limit_bytes=KERNEL_VMEM
        ),
    )(
        channel_input, norm_gain.reshape(1, width), routes.T, route_weight.T, log_decay,
        jnp.asarray(near), jnp.asarray(far), query_rows, key_rows, value_rows, gate_rows,
        out_weight, expert_gate, expert_up, expert_down, shared_gate, shared_up, shared_down,
    )
    return pl.pallas_call(
        hand_out, out_shape=tuple(jax.ShapeDtypeStruct(r.shape, r.dtype) for r in results),
        in_specs=[vmem] * 2, out_specs=(vmem, vmem),
    )(*results)


def hand_out(mixer_ref, channel_ref, mixer_out_ref, channel_out_ref):
    mixer_out_ref[...] = mixer_ref[...]
    channel_out_ref[...] = channel_ref[...]


def padded_bytes(shape, dtype):
    size = jnp.dtype(dtype).itemsize
    rows = 32 // size
    last = -(-shape[-1] // 128) * 128
    return math.prod(shape[:-2]) * (-(-shape[-2] // rows) * rows) * last * size


def one_kernel_fits(args, ep_count, chips, capacity):
    query_rows, log_decay, experts = args[0], args[4], args[10].shape[0] * ep_count
    heads = log_decay.shape[0]
    buffers, _ = whole_scratch(args, ep_count, chips, capacity)
    need = sum(padded_bytes(shape, dtype) for shape, dtype in buffers)
    return (
        chips > 1
        and capacity % 16 == 0
        and experts <= 128
        and experts * capacity <= 256
        and heads <= 8
        and query_rows.shape[1] // heads == 128
        and args[6].shape[0] % 16 == 0
        and need <= KERNEL_VMEM - (10 << 20)
    )


def local(
    query_rows, key_rows, value_rows, gate_rows, log_decay, out_weight, channel_input, norm_gain,
    routes, route_weight, expert_gate, expert_up, expert_down, shared_gate, shared_up, shared_down,
):
    ep_count, tp_count = lax.axis_size("ep"), lax.axis_size("tp")
    ep_index, tp_index = lax.axis_index("ep"), lax.axis_index("tp")
    chips = tp_count // CORES
    chip, core = tp_index // CORES, tp_index % CORES
    tokens_here, width = channel_input.shape
    topk = routes.shape[1]
    local_experts = expert_gate.shape[0]
    experts_all = ep_count * local_experts
    capacity = tokens_here * topk // experts_all + max(
        2, tokens_here * topk // (3 * experts_all)
    )

    args = (
        query_rows, key_rows, value_rows, gate_rows, log_decay, out_weight, channel_input,
        norm_gain, routes, route_weight, expert_gate, expert_up, expert_down, shared_gate,
        shared_up, shared_down,
    )
    if one_kernel_fits(args, ep_count, chips, capacity):
        return whole_step(args, ep_count, chips, capacity)

    wide = channel_input.astype(jnp.float32)
    normed = (
        wide * lax.rsqrt(jnp.mean(wide * wide, axis=-1, keepdims=True) + epsilon) * norm_gain
    ).astype(jnp.bfloat16)
    flat = routes.reshape(-1)
    onehot = (flat[:, None] == jnp.arange(experts_all, dtype=jnp.int32)[None, :]).astype(
        jnp.float32
    )
    count = tokens_here * topk
    before = (jnp.arange(count)[:, None] > jnp.arange(count)[None, :]).astype(jnp.float32)
    rank = jnp.sum(jnp.dot(before, onehot) * onehot, axis=1)
    notes = jnp.concatenate(
        [routes.astype(jnp.float32), rank.reshape(tokens_here, topk), route_weight], axis=1
    )
    notes = jnp.pad(notes, ((0, 0), (0, 128 - 3 * topk)))
    own_rows = line_gather(normed, chips)
    notes_all = line_gather(notes, chips)
    log_decay, normed, notes = lax.optimization_barrier((log_decay, normed, notes))
    route_all = notes_all[:, :, :topk].astype(jnp.int32)
    rank_all = notes_all[:, :, topk : 2 * topk].astype(jnp.int32)
    weight_all = notes_all[:, :, 2 * topk : 3 * topk]
    place = jnp.arange(chips, dtype=jnp.int32)[:, None, None]
    turn = (route_all // local_experts) ^ ep_index
    slot = ((turn * local_experts + route_all % local_experts) * chips + place) * capacity
    slot = (slot + rank_all).reshape(chips * tokens_here, topk)
    slot_count = experts_all * chips * capacity
    slot_ids = jnp.arange(slot_count, dtype=jnp.int32)
    placing = sum(
        (slot_ids[:, None] == slot[None, :, t]).astype(jnp.bfloat16) for t in range(topk)
    )
    own_flat = own_rows.reshape(chips * tokens_here, width)
    outgoing = jnp.dot(placing, own_flat, preferred_element_type=jnp.float32).astype(jnp.bfloat16)
    outgoing = outgoing.reshape(ep_count, local_experts, chips * capacity, width)
    arrived = [outgoing[0]] + [swap_ep(outgoing[k], k, ep_count) for k in range(1, ep_count)]
    own_twin = swap_cores(own_flat, tp_count)

    gated = retention(query_rows, key_rows, value_rows, gate_rows, log_decay)
    mixer_count = query_rows.shape[0] // tp_count
    gated_parts = gated.reshape(chips, CORES, mixer_count, gated.shape[1])

    def mixer_for(which):
        mine = lax.dynamic_index_in_dim(gated_parts, which, 1, keepdims=False)
        product = jnp.dot(
            mine.reshape(chips * mixer_count, -1), out_weight, preferred_element_type=jnp.float32
        )
        return product.astype(jnp.bfloat16)

    mixer_twin, mixer_mine = mixer_for(1 - core), mixer_for(core)
    mixer_half = summed(mixer_mine, swap_cores(mixer_twin, tp_count))
    arrived, _ = lax.optimization_barrier((arrived, (mixer_twin, mixer_mine)))
    arrived_twin = [swap_cores(block, tp_count) for block in arrived]
    mixer_half = mixer_half.reshape(chips, mixer_count, width)
    mixer_out = line_scatter(
        lambda r: lax.dynamic_index_in_dim(mixer_half, (chip + r) % chips, 0, False), chips
    ).astype(jnp.bfloat16)

    def experts_on(blocks, rows):
        routed = jnp.concatenate(blocks, axis=1)
        gate_part = jnp.einsum("emd,edf->emf", routed, expert_gate, preferred_element_type=jnp.float32)
        up_part = jnp.einsum("emd,edf->emf", routed, expert_up, preferred_element_type=jnp.float32)
        hidden = gated_pair(gate_part, up_part)
        routed_term = jnp.einsum(
            "emf,efd->emd", hidden, expert_down, preferred_element_type=jnp.float32
        ).astype(jnp.bfloat16)
        shared_hidden = gated_pair(
            jnp.dot(rows, shared_gate, preferred_element_type=jnp.float32),
            jnp.dot(rows, shared_up, preferred_element_type=jnp.float32),
        )
        shared_term = jnp.dot(
            shared_hidden, shared_down, preferred_element_type=jnp.float32
        ).astype(jnp.bfloat16)
        return routed_term, shared_term

    routed_twin, shared_twin = experts_on(arrived_twin, own_twin)
    routed_mine, shared_mine = experts_on(arrived, own_flat)
    routed = summed(routed_mine, swap_cores(routed_twin, tp_count))
    shared = summed(shared_mine, swap_cores(shared_twin, tp_count))
    routed = routed.reshape(local_experts, ep_count, chips * capacity, width)
    returned = [routed[:, 0]] + [swap_ep(routed[:, k], k, ep_count) for k in range(1, ep_count)]
    returned = jnp.stack(returned).reshape(slot_count, width)
    flat_weight = weight_all.reshape(chips * tokens_here, topk)
    mixing = sum(
        jnp.where(slot_ids[None, :] == slot[:, t : t + 1], flat_weight[:, t : t + 1], 0.0)
        for t in range(topk)
    )
    coarse = lax.reduce_precision(mixing, 8, 7)
    fine = (mixing - coarse).astype(jnp.bfloat16)
    coarse = coarse.astype(jnp.bfloat16)
    channel = (
        jnp.dot(coarse, returned, preferred_element_type=jnp.float32)
        + jnp.dot(fine, returned, preferred_element_type=jnp.float32)
        + shared.astype(jnp.float32)
    ).astype(jnp.bfloat16)
    channel = channel.reshape(chips, tokens_here, width)
    channel_out = line_scatter(lambda r: channel[(chips - r) % chips], chips).astype(jnp.bfloat16)
    return (mixer_out, channel_out)


def solution(mesh):
    in_specs = (
        P("ep", "tp"),
        P("ep", "tp"),
        P("ep", "tp"),
        P("ep", "tp"),
        P("tp", "ep"),
        P("tp", None),
        P(("ep", "tp"), None),
        P(),
        P(("ep", "tp"), None),
        P(("ep", "tp"), None),
        P("ep", None, "tp"),
        P("ep", None, "tp"),
        P("ep", "tp", None),
        P(None, "tp"),
        P(None, "tp"),
        P("tp", None),
    )
    out_specs = (P(("ep", "tp"), None), P(("ep", "tp"), None))
    return jax.shard_map(local, mesh=mesh, in_specs=in_specs, out_specs=out_specs, check_vma=False)
```

```python
import functools
import math

import jax
import jax.numpy as jnp
import numpy as np
from jax import lax
from jax.experimental import pallas as pl
from jax.experimental.pallas import tpu as pltpu
from jax.sharding import PartitionSpec as P

BLOCK = 128
CORES = 2
KERNEL_VMEM = 67043328

epsilon = 1e-06
turn_base = 10000.0


def shift_chips(array, r, count):
    pairs = [
        (z * CORES + c, (z + r) % count * CORES + c) for z in range(count) for c in range(CORES)
    ]
    return lax.ppermute(array, "tp", pairs)


def line_gather(array, count):
    return jnp.stack([array] + [shift_chips(array, r, count) for r in range(1, count)])


def line_scatter(part, count):
    total = part(0).astype(jnp.float32)
    for r in range(1, count):
        total = total + shift_chips(part(r), r, count).astype(jnp.float32)
    return total


def swap_cores(array, tp_count):
    return lax.ppermute(array, "tp", [(i, i ^ 1) for i in range(tp_count)])


def swap_ep(array, k, ep_count):
    return lax.ppermute(array, "ep", [(i, i ^ k) for i in range(ep_count)])


def turned(rows, cosine, sine):
    wide = rows.astype(jnp.float32)
    return (wide * cosine + pltpu.roll(wide, wide.shape[1] // 2, 1) * sine).astype(jnp.bfloat16)


def state_kernel(key_ref, value_ref, cosine_ref, sine_ref, fade_ref, state_ref):
    heads, key_width, value_width = state_ref.shape
    for h in range(heads):
        keys = turned(
            key_ref[:, h * key_width : (h + 1) * key_width], cosine_ref[...], sine_ref[...]
        )
        faded = (keys.astype(jnp.float32) * fade_ref[:, h : h + 1]).astype(jnp.bfloat16)
        state_ref[h] = lax.dot_general(
            faded,
            value_ref[:, h * value_width : (h + 1) * value_width],
            (((0,), (0,)), ((), ())),
            preferred_element_type=jnp.float32,
        ).astype(state_ref.dtype)


def retention_kernel(
    query_ref, key_ref, value_ref, gate_ref, cosine_ref, sine_ref, column_ref, row_ref,
    entry_ref, out_ref, state,
):
    heads, key_width, value_width = state.shape

    @pl.when(pl.program_id(0) == 0)
    def _():
        state[...] = entry_ref[...]

    cosine, sine = cosine_ref[...], sine_ref[...]
    lower = lax.broadcasted_iota(jnp.int32, (BLOCK, BLOCK), 0) >= lax.broadcasted_iota(
        jnp.int32, (BLOCK, BLOCK), 1
    )
    for h in range(heads):
        key_cut = slice(h * key_width, (h + 1) * key_width)
        value_cut = slice(h * value_width, (h + 1) * value_width)
        queries = turned(query_ref[:, key_cut], cosine, sine)
        keys = turned(key_ref[:, key_cut], cosine, sine)
        values = value_ref[:, value_cut]
        column = column_ref[:, h : h + 1]
        row = row_ref[0, h : h + 1, :]
        end = column_ref[BLOCK - 1 : BLOCK, h : h + 1]
        scores = lax.dot_general(
            queries, keys, (((1,), (1,)), ((), ())), preferred_element_type=jnp.float32
        )
        spread = jnp.exp(jnp.where(lower, column - row, 0.0))
        weights = jnp.where(lower, scores * spread, 0.0).astype(jnp.bfloat16)
        before = state[h]
        retained = jnp.dot(weights, values, preferred_element_type=jnp.float32)
        retained = retained + jnp.exp(column) * jnp.dot(
            queries, before.astype(jnp.bfloat16), preferred_element_type=jnp.float32
        )
        faded = (keys.astype(jnp.float32) * jnp.exp(end - column)).astype(jnp.bfloat16)
        state[h] = jnp.exp(end) * before + lax.dot_general(
            faded, values, (((0,), (0,)), ((), ())), preferred_element_type=jnp.float32
        )
        scale = lax.rsqrt(jnp.mean(retained * retained, axis=1, keepdims=True) + epsilon)
        gate = gate_ref[:, value_cut].astype(jnp.float32)
        out_ref[:, value_cut] = (gate / (1.0 + jnp.exp(-gate)) * (retained * scale)).astype(
            jnp.bfloat16
        )


def retention(query_rows, key_rows, value_rows, gate_rows, log_decay):
    tokens = query_rows.shape[0]
    heads = log_decay.shape[0]
    key_width = query_rows.shape[1] // heads
    value_width = value_rows.shape[1] // heads
    blocks = tokens // BLOCK
    ep_count, ep_index = lax.axis_size("ep"), lax.axis_index("ep")
    half = key_width // 2
    position = (ep_index * tokens + jnp.arange(tokens, dtype=jnp.int32)).astype(jnp.float32)
    inverse = turn_base ** (-jnp.arange(half, dtype=jnp.float32) / half)
    angles = position[:, None] * inverse[None, :]
    cosine, sine = jnp.cos(angles), jnp.sin(angles)
    cosine = jnp.concatenate([cosine, cosine], axis=1)
    sine = jnp.concatenate([-sine, sine], axis=1)
    running = jnp.cumsum(log_decay.reshape(heads, blocks, BLOCK), axis=2)
    ends = running[:, :, -1]
    later = jnp.sum(ends, axis=1, keepdims=True) - jnp.cumsum(ends, axis=1)
    later = jnp.minimum(later, 0.0)
    fade = jnp.exp(ends[:, :, None] - running + later[:, :, None]).reshape(heads, tokens).T
    total = jnp.sum(ends, axis=1)
    vmem = pl.BlockSpec(memory_space=pltpu.VMEM)
    own_state = pl.pallas_call(
        state_kernel,
        out_shape=jax.ShapeDtypeStruct((heads, key_width, value_width), jnp.bfloat16),
        in_specs=[vmem] * 5,
        out_specs=vmem,
        cost_estimate=pl.CostEstimate(
            flops=2 * tokens * heads * key_width * value_width * 4,
            bytes_accessed=8 << 20,
            transcendentals=0,
        ),
    )(key_rows, value_rows, cosine, sine, fade)
    totals_sent = jnp.broadcast_to(total[:, None], (heads, 128))
    states, totals = [], [total]
    for k in range(1, ep_count):
        states.append(swap_ep(own_state, k, ep_count))
        totals.append(swap_ep(totals_sent, k, ep_count)[:, 0])
    entry = jnp.zeros((heads, key_width, value_width), jnp.float32)
    for k in range(1, ep_count):
        source = ep_index ^ k
        passed = jnp.zeros_like(total)
        for m in range(1, ep_count):
            between = ((ep_index ^ m) > source) & ((ep_index ^ m) < ep_index)
            passed = passed + jnp.where(between, totals[m], 0.0)
        share = jnp.where(source < ep_index, jnp.exp(passed), 0.0)
        entry = entry + share[:, None, None] * states[k - 1].astype(jnp.float32)
    columns = running.reshape(heads, tokens).T
    rows = running.transpose(1, 0, 2)
    by_block = lambda width: pl.BlockSpec((BLOCK, width), lambda n: (n, 0))
    whole = pl.BlockSpec((heads, key_width, value_width), lambda n: (0, 0, 0))
    return pl.pallas_call(
        retention_kernel,
        out_shape=jax.ShapeDtypeStruct((tokens, heads * value_width), jnp.bfloat16),
        grid=(blocks,),
        in_specs=[
            by_block(heads * key_width),
            by_block(heads * key_width),
            by_block(heads * value_width),
            by_block(heads * value_width),
            by_block(key_width),
            by_block(key_width),
            by_block(heads),
            pl.BlockSpec((1, heads, BLOCK), lambda n: (n, 0, 0)),
            whole,
        ],
        out_specs=by_block(heads * value_width),
        scratch_shapes=[pltpu.VMEM((heads, key_width, value_width), jnp.float32)],
        cost_estimate=pl.CostEstimate(
            flops=8 << 30, bytes_accessed=24 << 20, transcendentals=0
        ),
    )(query_rows, key_rows, value_rows, gate_rows, cosine, sine, columns, rows, entry)


def gated_pair(gate_part, up_part):
    return (jax.nn.silu(gate_part) * up_part).astype(jnp.bfloat16)


def summed(a, b):
    return (a.astype(jnp.float32) + b.astype(jnp.float32)).astype(jnp.bfloat16)


def flip(index, k):
    turned_index, bit = index, 1
    while bit <= k:
        if k & bit:
            turned_index = turned_index + bit - 2 * bit * ((index // bit) % 2)
        bit *= 2
    return turned_index


def line_order(chips):
    orders = []
    for z in range(chips):
        right, left = list(range(chips - 1, z, -1)), list(range(z))
        order = []
        sides = [right, left] if len(right) >= len(left) else [left, right]
        while right or left:
            if sides[0]:
                order.append(sides[0].pop(0))
            sides.reverse()
        orders.append(order + [z])
    return orders


def arrival_order(chips):
    def rank(z, q):
        hands_on = (q <= z - 2 and z < chips - 1) or (q >= z + 2 and z > 0)
        return (not hands_on, abs(q - z), q)

    return [
        sorted((q for q in range(chips) if q != z), key=functools.partial(rank, z))
        for z in range(chips)
    ]


def pick(table, index):
    chosen = 0
    for i, entry in enumerate(table):
        chosen = chosen + jnp.where(index == i, entry, 0)
    return chosen


def in_steps(count, together, body):
    together = math.gcd(count, together)

    def step(i, carry):
        for j in range(together):
            body(i * together + j)
        return carry

    lax.fori_loop(0, count // together, step, 0)


def whole_kernel(
    sizes,
    channel_ref, gain_ref, routes_ref, weight_ref, decay_ref, near_ref, far_ref,
    query_any, key_any, value_any, gate_any, out_any, eg_any, eu_any, ed_any, sg_any, su_any,
    sd_any,
    mixer_ref, channel_out_ref,
    query, key, value, gate, out_w, eg, eu, ed, sg, su, sd,
    gathered, slots, arrived, result_twin, result_in, result, returned,
    shared_twin, shared_in, shared_own, channel, channel_right, channel_left,
    mix_twin, mix_in, mix_own, mix_right, mix_left,
    gated, partial, keys_turned, before, entry, state_send, state_in, total_send, total_in, prefix,
    decay_flat, run_row, run_col,
    local_sem, g_send, g_recv, f_send, tg_send, tg_recv, d_send, d_recv, ta_send, ta_recv,
    ty_send, ty_recv, th_send, th_recv, r_send, r_recv, s_send, s_recv, o_send, o_recv,
    tp_send, tp_recv, m_send, m_right, m_left, c_send, c_right, c_left,
):
    ep_count, chips, capacity = sizes
    f32, bf16 = jnp.float32, jnp.bfloat16
    tokens_here, width = channel_ref.shape
    topk = routes_ref.shape[0]
    local_experts = eg.shape[0]
    block_rows = local_experts * capacity
    slot_count = ep_count * block_rows
    heads, key_width, value_width = entry.shape
    blocks = before.shape[0]
    mixer_count = mixer_ref.shape[0]
    ep_index, tp_index = lax.axis_index("ep"), lax.axis_index("tp")
    chip, core = tp_index // CORES, tp_index % CORES
    twin = tp_index + 1 - 2 * core
    orders = line_order(chips)
    order = [pick([row[i] for row in orders], chip) for i in range(chips - 1)] + [chip]
    arrivals = arrival_order(chips)
    arrival = [pick([row[i] for row in arrivals], chip) for i in range(chips - 1)]

    def to_tp(src, dst, send, recv, target):
        return pltpu.make_async_remote_copy(
            src_ref=src, dst_ref=dst, send_sem=send, recv_sem=recv,
            device_id={"tp": target}, device_id_type=pl.DeviceIdType.MESH,
        )

    def to_ep(src, dst, send, recv, target):
        return pltpu.make_async_remote_copy(
            src_ref=src, dst_ref=dst, send_sem=send, recv_sem=recv,
            device_id={"ep": target}, device_id_type=pl.DeviceIdType.MESH,
        )

    barrier = pltpu.get_barrier_semaphore()
    for r in range(1, chips):
        pl.semaphore_signal(
            barrier, inc=1, device_id={"tp": (chip + r) % chips * CORES + core},
            device_id_type=pl.DeviceIdType.MESH,
        )
    pl.semaphore_signal(
        barrier, inc=1, device_id={"tp": twin}, device_id_type=pl.DeviceIdType.MESH
    )
    for k in range(1, ep_count):
        pl.semaphore_signal(
            barrier, inc=1, device_id={"ep": flip(ep_index, k)},
            device_id_type=pl.DeviceIdType.MESH,
        )

    pairs = [
        (key_any, key), (value_any, value), (query_any, query), (gate_any, gate),
        (out_any, out_w), (sg_any, sg), (su_any, su), (sd_any, sd), (eg_any, eg), (eu_any, eu),
        (ed_any, ed),
    ]
    loads = [pltpu.make_async_copy(s, d, local_sem.at[i]) for i, (s, d) in enumerate(pairs)]
    for load in loads:
        load.start()

    wide = channel_ref[...].astype(f32)
    normed = (
        wide * lax.rsqrt(jnp.mean(wide * wide, axis=-1, keepdims=True) + epsilon) * gain_ref[...]
    ).astype(bf16)
    gathered[chip, 0, :, :width] = normed
    lane = lax.broadcasted_iota(jnp.int32, (tokens_here, 128), 1)
    same = (
        lax.broadcasted_iota(jnp.int32, (tokens_here, tokens_here), 0)
        == lax.broadcasted_iota(jnp.int32, (tokens_here, tokens_here), 1)
    ).astype(f32)

    def as_columns(rows):
        return lax.dot_general(
            same, rows, (((1,), (1,)), ((), ())), preferred_element_type=f32,
            precision=lax.Precision.HIGHEST,
        )

    route_columns = as_columns(routes_ref[...].astype(f32))
    weight_columns = as_columns(weight_ref[...])
    routed_to = [route_columns[:, t : t + 1] for t in range(topk)]
    named = [(route == lane.astype(f32)).astype(f32) for route in routed_to]
    earlier = (
        lax.broadcasted_iota(jnp.int32, (tokens_here, tokens_here), 0)
        > lax.broadcasted_iota(jnp.int32, (tokens_here, tokens_here), 1)
    ).astype(bf16)
    ahead = jnp.dot(earlier, sum(named).astype(bf16), preferred_element_type=f32)
    noted = jnp.zeros((tokens_here, 128), f32)
    for t in range(topk):
        rank = jnp.sum(ahead * named[t], axis=1, keepdims=True)
        noted = jnp.where(lane == t, routed_to[t] * capacity + rank, noted)
        left = weight_columns[:, t : t + 1]
        for piece in range(3):
            term = left.astype(bf16).astype(f32)
            noted = jnp.where(lane == topk + 3 * t + piece, term, noted)
            left = left - term
    gathered[chip, 0, :, width:] = noted.astype(bf16)

    def slot_of(q, t):
        return gathered[q, 0, :, width:].astype(f32)[:, t : t + 1]

    def weight_of(q, t):
        terms = gathered[q, 0, :, width:].astype(f32)
        at = topk + 3 * t
        return terms[:, at : at + 1] + terms[:, at + 1 : at + 2] + terms[:, at + 2 : at + 3]

    pl.semaphore_wait(barrier, chips + ep_count - 1)

    def gather_row(q, target):
        return to_tp(
            gathered.at[q, 0], gathered.at[q, 0], g_send.at[target], g_recv.at[q],
            target * CORES + core,
        )

    def relay_row(q, target):
        return to_tp(
            gathered.at[q, 0], gathered.at[q, 0], f_send.at[q], g_recv.at[q],
            target * CORES + core,
        )

    def relay(q, act):
        @pl.when((q <= chip - 2) & (chip < chips - 1))
        def _():
            act(relay_row(q, chip + 1))

        @pl.when((q >= chip + 2) & (chip > 0))
        def _():
            act(relay_row(q, chip - 1))

    def twin_row(q):
        return to_tp(
            gathered.at[q, 0], gathered.at[q, 1], tg_send.at[q], tg_recv.at[q], twin
        )

    def reached(target):
        return (target - chip) * (target - chip) <= 4

    for target in order[:-1]:
        @pl.when(reached(target))
        def _():
            gather_row(chip, target).start()

    twin_row(chip).start()

    slot_lane = lax.broadcasted_iota(jnp.int32, (tokens_here, slot_count), 1).astype(f32)

    def dispatch_copy(q, k):
        target = flip(ep_index, k)
        return to_ep(
            slots.at[q, target], arrived.at[q, 0, ep_index], d_send.at[q, k], d_recv.at[q, k],
            target,
        )

    def dispatch(q):
        placing = sum(
            (slot_of(q, t) == slot_lane).astype(f32) for t in range(topk)
        ).astype(bf16)
        rows = lax.dot_general(
            placing, gathered[q, 0, :, :width], (((0,), (0,)), ((), ())), preferred_element_type=f32
        ).astype(bf16)
        slots[q] = rows.reshape(ep_count, block_rows, width)
        for k in range(1, ep_count):
            dispatch_copy(q, k).start()
        arrived[q, 0, ep_index] = slots[q, ep_index]

    def take_row(q):
        gather_row(q, q).wait_recv()
        relay(q, lambda copy: copy.start())
        twin_row(q).start()
        dispatch(q)

    for n in range(blocks):
        decay_flat[n * heads : (n + 1) * heads, :] = decay_ref[:, n * BLOCK : (n + 1) * BLOCK]
    upper = (
        lax.broadcasted_iota(jnp.int32, (BLOCK, BLOCK), 0)
        <= lax.broadcasted_iota(jnp.int32, (BLOCK, BLOCK), 1)
    )
    lower = (
        lax.broadcasted_iota(jnp.int32, (BLOCK, BLOCK), 0)
        >= lax.broadcasted_iota(jnp.int32, (BLOCK, BLOCK), 1)
    )
    flat = decay_flat[...]
    by_row = jnp.dot(
        flat, upper.astype(f32), preferred_element_type=f32, precision=lax.Precision.HIGHEST
    )
    by_col = lax.dot_general(
        lower.astype(f32), flat, (((1,), (1,)), ((), ())), preferred_element_type=f32,
        precision=lax.Precision.HIGHEST,
    )
    for n in range(blocks):
        run_row[n] = jnp.zeros(run_row.shape[1:], f32)
        run_row[n, 0:heads, :] = by_row[n * heads : (n + 1) * heads, :]
        run_col[n, :, 0:heads] = by_col[:, n * heads : (n + 1) * heads]

    def turns(n):
        far = far_ref[ep_index * blocks + n]
        far_cos, far_sin = far[0:1, :], far[1:2, :]
        near_cos, near_sin = near_ref[0], near_ref[1]
        return near_cos * far_cos - near_sin * far_sin, near_sin * far_cos + near_cos * far_sin

    whole_decay = jnp.zeros(total_send.shape, f32)
    for n in range(blocks):
        prefix[n] = whole_decay
        whole_decay = whole_decay + run_row[n, :, BLOCK - 1 : BLOCK]
    total_send[...] = whole_decay

    def state_copy(k, h):
        return to_ep(
            state_send.at[h], state_in.at[k, h], s_send.at[k, h], s_recv.at[k, h],
            flip(ep_index, k),
        )

    def total_copy(k):
        return to_ep(
            total_send, total_in.at[k], o_send.at[k], o_recv.at[k], flip(ep_index, k)
        )

    for k in range(1, ep_count):
        @pl.when(flip(ep_index, k) > ep_index)
        def _():
            total_copy(k).start()

    loads[0].wait()
    loads[1].wait()

    def first_pass(h):
        key_cut = slice(h * key_width, (h + 1) * key_width)
        value_cut = slice(h * value_width, (h + 1) * value_width)
        held = jnp.zeros((key_width, value_width), f32)
        for n in range(blocks):
            at = slice(n * BLOCK, (n + 1) * BLOCK)
            keys = turned(key[at, key_cut], *turns(n))
            keys_turned[at, key_cut] = keys
            end = run_row[n, h : h + 1, BLOCK - 1 : BLOCK]
            faded = (keys.astype(f32) * jnp.exp(end - run_col[n, :, h : h + 1])).astype(bf16)
            before[n, h] = held
            held = jnp.exp(end) * held + lax.dot_general(
                faded, value[at, value_cut], (((0,), (0,)), ((), ())),
                preferred_element_type=f32,
            )
        state_send[h] = held.astype(bf16)

    for h in range(heads):
        first_pass(h)
        for k in range(1, ep_count):
            @pl.when(flip(ep_index, k) > ep_index)
            def _():
                state_copy(k, h).start()

    loads[2].wait()

    def second_pass(n):
        at = pl.ds(pl.multiple_of(n * BLOCK, BLOCK), BLOCK)
        cosine, sine = turns(n)
        for h in range(heads):
            key_cut = slice(h * key_width, (h + 1) * key_width)
            value_cut = slice(h * value_width, (h + 1) * value_width)
            queries = turned(query[at, key_cut], cosine, sine)
            query[at, key_cut] = queries
            column = run_col[n, :, h : h + 1]
            row = run_row[n, h : h + 1, :]
            scores = lax.dot_general(
                queries, keys_turned[at, key_cut], (((1,), (1,)), ((), ())),
                preferred_element_type=f32,
            )
            spread = jnp.exp(jnp.where(lower, column - row, 0.0))
            weights = jnp.where(lower, scores * spread, 0.0).astype(bf16)
            partial[at, value_cut] = jnp.dot(
                weights, value[at, value_cut], preferred_element_type=f32
            ) + jnp.exp(column) * jnp.dot(
                queries, before[n, h].astype(bf16), preferred_element_type=f32
            )

    in_steps(blocks, 2, second_pass)
    take_row(arrival[0])

    loads[3].wait()
    for k in range(1, ep_count):
        @pl.when(flip(ep_index, k) < ep_index)
        def _():
            total_copy(k).wait_recv()

        @pl.when(flip(ep_index, k) > ep_index)
        def _():
            total_in[k] = jnp.zeros_like(total_send)
            state_in[k] = jnp.zeros_like(state_send)

    shares = []
    for k in range(1, ep_count):
        source = flip(ep_index, k)
        passed = jnp.zeros(total_send.shape, f32)
        for m in range(1, ep_count):
            between = (flip(ep_index, m) > source) & (flip(ep_index, m) < ep_index)
            passed = passed + jnp.where(between, total_in[m], 0.0)
        shares.append(jnp.where(source < ep_index, jnp.exp(passed), 0.0))

    def third_pass(h):
        for k in range(1, ep_count):
            @pl.when(flip(ep_index, k) < ep_index)
            def _():
                state_copy(k, h).wait_recv()

        entry[h] = sum(
            shares[k - 1][h : h + 1, 0:1] * state_in[k, h].astype(f32)
            for k in range(1, ep_count)
        )
        value_cut = slice(h * value_width, (h + 1) * value_width)

        def finish(n):
            at = pl.ds(pl.multiple_of(n * BLOCK, BLOCK), BLOCK)
            grown = jnp.exp(run_col[n, :, h : h + 1] + prefix[n, h : h + 1, 0:1])
            retained = partial[at, value_cut] + grown * jnp.dot(
                query[at, h * key_width : (h + 1) * key_width], entry[h].astype(bf16),
                preferred_element_type=f32,
            )
            scale = lax.rsqrt(jnp.mean(retained * retained, axis=1, keepdims=True) + epsilon)
            gates = gate[at, value_cut].astype(f32)
            gated[at, value_cut] = (
                gates / (1.0 + jnp.exp(-gates)) * (retained * scale)
            ).astype(bf16)

        in_steps(blocks, 4, finish)

    for h in range(heads):
        third_pass(h)

    loads[4].wait()

    def twin_mix(d):
        return to_tp(mix_twin.at[d], mix_in.at[d], tp_send.at[d], tp_recv.at[d], twin)

    def project(d, which, into):
        start = pl.multiple_of((d * CORES + which) * mixer_count, mixer_count)
        into[d] = jnp.dot(
            gated[pl.ds(start, mixer_count), :], out_w[...], preferred_element_type=f32
        ).astype(bf16)

    def mix_copy(d, half, step, target):
        rows = pl.ds(half * (mixer_count // 2), mixer_count // 2)
        return to_tp(
            mix_own.at[d, rows], (mix_right if step > 0 else mix_left).at[d, rows],
            m_send.at[d, half], (m_right if step > 0 else m_left).at[d, half], target,
        )

    def mix_step(d, half, step):
        return mix_copy(d, half, step, (chip + step) * CORES + core)

    def mix_wait(d, half, step):
        return mix_copy(d, half, step, twin)

    def mix_sum(d, half, *others):
        rows = pl.ds(half * (mixer_count // 2), mixer_count // 2)
        total = mix_own[d, rows].astype(f32) + mix_in[d, rows].astype(f32)
        for other in others:
            total = total + other[d, rows].astype(f32)
        mix_own[d, rows] = total.astype(bf16)

    def mix_lead(d, halves):
        @pl.when((chip == 0) | (chip == chips - 1))
        def _():
            for half in halves:
                mix_sum(d, half)

        @pl.when(chip == 0)
        def _():
            for half in halves:
                mix_step(d, half, 1).start()

        @pl.when(chip == chips - 1)
        def _():
            for half in halves:
                mix_step(d, half, -1).start()

    def mix_follow(d, half):
        @pl.when((chip > 0) & (d > chip))
        def _():
            mix_wait(d, half, 1).wait_recv()
            mix_sum(d, half, mix_right)
            mix_step(d, half, 1).start()

        @pl.when((chip < chips - 1) & (d < chip))
        def _():
            mix_wait(d, half, -1).wait_recv()
            mix_sum(d, half, mix_left)
            mix_step(d, half, -1).start()

    def channel_step(d, step):
        return to_tp(
            channel.at[d], (channel_right if step > 0 else channel_left).at[d], c_send.at[d],
            (c_right if step > 0 else c_left).at[d], (chip + step) * CORES + core,
        )

    def channel_wait(d, step):
        return to_tp(
            channel.at[d], (channel_right if step > 0 else channel_left).at[d], c_send.at[d],
            (c_right if step > 0 else c_left).at[d], twin,
        )

    def project_twin(d):
        project(d, 1 - core, mix_twin)
        twin_mix(d).start()

    project_twin(order[0])
    rows_left = arrival[1:]
    for i, d in enumerate(order[:-1]):
        project_twin(order[i + 1])
        project(d, core, mix_own)
        twin_mix(d).wait_recv()
        mix_lead(d, (0, 1) if i + 2 < chips else (0,))
        for q in rows_left[:1] if i == 0 else rows_left if i + 2 == chips else ():
            take_row(q)
            rows_left = rows_left[1:]
    project(chip, core, mix_own)

    for load in loads[5:]:
        load.wait()

    def twin_arrived(q):
        return to_tp(arrived.at[q, 0], arrived.at[q, 1], ta_send.at[q], ta_recv.at[q], twin)

    def twin_result(q):
        return to_tp(
            result_twin.at[q], result_in.at[q], ty_send.at[q], ty_recv.at[q], twin
        )

    def twin_shared(q):
        return to_tp(
            shared_twin.at[q], shared_in.at[q], th_send.at[q], th_recv.at[q], twin
        )

    def return_copy(q, k):
        target = flip(ep_index, k)
        return to_ep(
            result.at[q, target], returned.at[q, ep_index], r_send.at[q, k], r_recv.at[q, k],
            target,
        )

    def hand_over(q):
        for k in range(1, ep_count):
            dispatch_copy(q, k).wait_recv()
        twin_arrived(q).start()

    def gated_rows(rows, gate_weight, up_weight):
        gate_part = jnp.dot(rows, gate_weight, preferred_element_type=f32)
        up_part = jnp.dot(rows, up_weight, preferred_element_type=f32)
        return (gate_part / (1.0 + jnp.exp(-gate_part)) * up_part).astype(bf16)

    def shared(q):
        twin_row(q).wait_recv()
        rows = gathered[q, :, :, :width].reshape(CORES * tokens_here, width)
        hidden = gated_rows(rows, sg[...], su[...])
        product = jnp.dot(hidden, sd[...], preferred_element_type=f32).astype(bf16)
        shared_own[q] = product[:tokens_here]
        shared_twin[q] = product[tokens_here:]
        twin_shared(q).start()

    def experts(q):
        twin_arrived(q).wait_recv()
        for j in range(local_experts):
            cut = slice(j * capacity, (j + 1) * capacity)
            rows = arrived[q, :, :, cut, :].reshape(CORES * ep_count * capacity, width)
            hidden = gated_rows(rows, eg[j], eu[j])
            product = jnp.dot(hidden, ed[j], preferred_element_type=f32).astype(bf16)
            product = product.reshape(CORES, ep_count, capacity, width)
            result[q, :, cut, :] = product[0]
            result_twin[q, :, cut, :] = product[1]
        twin_result(q).start()

    def give_back(q):
        twin_result(q).wait_recv()
        result[q] = (result[q].astype(f32) + result_in[q].astype(f32)).astype(bf16)
        for k in range(1, ep_count):
            return_copy(q, k).start()
        returned[q, ep_index] = result[q, ep_index]

    others = order[:-1]
    for q in arrival + [chip]:
        shared(q)
    dispatch(chip)
    for half in range(2):
        mix_follow(others[0], half)
    for q in others[:0:-1]:
        hand_over(q)
    for q in others[:0:-1]:
        experts(q)
    hand_over(others[0])
    experts(others[0])
    for q in others[:-1]:
        give_back(q)
    hand_over(chip)
    for d in others[1:]:
        mix_follow(d, 0)
    give_back(others[-1])
    experts(chip)
    for d in others[1:]:
        mix_follow(d, 1)
    give_back(chip)

    def combined(q):
        for k in range(1, ep_count):
            return_copy(q, k).wait_recv()
        twin_shared(q).wait_recv()
        mixing = sum(
            jnp.where(
                slot_of(q, t) == slot_lane, weight_of(q, t), 0.0
            )
            for t in range(topk)
        )
        coarse = mixing.astype(bf16)
        fine = (mixing - coarse.astype(f32)).astype(bf16)
        rows = returned[q].reshape(slot_count, width)
        return (
            jnp.dot(coarse, rows, preferred_element_type=f32)
            + jnp.dot(fine, rows, preferred_element_type=f32)
            + shared_own[q].astype(f32)
            + shared_in[q].astype(f32)
        )

    def channel_on(d):
        own = combined(d)
        from_left = (chip > 0) & (d > chip)
        from_right = (chip < chips - 1) & (d < chip)

        @pl.when(from_left)
        def _():
            channel_wait(d, 1).wait_recv()
            channel[d] = (own + channel_right[d].astype(f32)).astype(bf16)

        @pl.when(from_right)
        def _():
            channel_wait(d, -1).wait_recv()
            channel[d] = (own + channel_left[d].astype(f32)).astype(bf16)

        @pl.when((chip == 0) | (chip == chips - 1))
        def _():
            channel[d] = own.astype(bf16)

        @pl.when(d > chip)
        def _():
            channel_step(d, 1).start()

        @pl.when(d < chip)
        def _():
            channel_step(d, -1).start()

    for i, d in enumerate(order[:-1]):
        channel_on(d)
        if i == 0:
            mix_lead(order[-2], (1,))

    def line_end(own, right_waits, left_waits, right_buffer, left_buffer, into):
        into[chip] = own.astype(bf16)

        @pl.when(chip > 0)
        def _():
            for wait in right_waits:
                wait.wait_recv()

        @pl.when(chip < chips - 1)
        def _():
            for wait in left_waits:
                wait.wait_recv()

        @pl.when((chip > 0) & (chip < chips - 1))
        def _():
            into[chip] = (
                own + right_buffer[chip].astype(f32) + left_buffer[chip].astype(f32)
            ).astype(bf16)

        @pl.when(chip == chips - 1)
        def _():
            into[chip] = (own + right_buffer[chip].astype(f32)).astype(bf16)

        @pl.when(chip == 0)
        def _():
            into[chip] = (own + left_buffer[chip].astype(f32)).astype(bf16)

    twin_mix(chip).wait_recv()
    line_end(
        mix_own[chip].astype(f32) + mix_in[chip].astype(f32),
        [mix_wait(chip, half, 1) for half in range(2)],
        [mix_wait(chip, half, -1) for half in range(2)], mix_right, mix_left, mix_own,
    )
    mixer_store = pltpu.make_async_copy(mix_own.at[chip], mixer_ref, local_sem.at[len(pairs)])
    mixer_store.start()
    line_end(
        combined(chip), [channel_wait(chip, 1)], [channel_wait(chip, -1)], channel_right,
        channel_left, channel,
    )
    channel_store = pltpu.make_async_copy(
        channel.at[chip], channel_out_ref, local_sem.at[len(pairs) + 1]
    )
    channel_store.start()

    for d in order[:-1]:
        @pl.when(reached(d))
        def _():
            gather_row(chip, d).wait_send()

        relay(d, lambda copy: copy.wait_send())
        mix_wait(d, 0, 1).wait_send()
        mix_wait(d, 1, 1).wait_send()
        channel_wait(d, 1).wait_send()
    for q in range(chips):
        twin_row(q).wait_send()
        twin_mix(q).wait_send()
        twin_arrived(q).wait_send()
        twin_result(q).wait_send()
        twin_shared(q).wait_send()
        for k in range(1, ep_count):
            dispatch_copy(q, k).wait_send()
            return_copy(q, k).wait_send()
    for k in range(1, ep_count):
        @pl.when(flip(ep_index, k) > ep_index)
        def _():
            total_copy(k).wait_send()
            for h in range(heads):
                state_copy(k, h).wait_send()

    mixer_store.wait()
    channel_store.wait()


def turn_tables(key_width, sequence):
    half = key_width // 2
    inverse = np.float32(turn_base) ** (-np.arange(half, dtype=np.float32) / np.float32(half))
    inverse = inverse.astype(np.float64)

    def both(positions):
        angles = positions[:, None].astype(np.float64) * inverse[None, :]
        cosine, sine = np.cos(angles), np.sin(angles)
        return np.stack(
            [np.concatenate([cosine, cosine], axis=1), np.concatenate([-sine, sine], axis=1)]
        ).astype(np.float32)

    near = both(np.arange(BLOCK))
    far = both(np.arange(sequence // BLOCK) * BLOCK).transpose(1, 0, 2)
    return near, far


def whole_scratch(args, ep_count, chips, capacity):
    (
        query_rows, key_rows, value_rows, gate_rows, log_decay, out_weight, channel_input,
        _, _, _, expert_gate, expert_up, expert_down, shared_gate, shared_up, shared_down,
    ) = args
    f32, bf16 = jnp.float32, jnp.bfloat16
    tokens_here, width = channel_input.shape
    tokens, heads = query_rows.shape[0], log_decay.shape[0]
    key_width = query_rows.shape[1] // heads
    value_width = value_rows.shape[1] // heads
    blocks = tokens // BLOCK
    block_rows = expert_gate.shape[0] * capacity
    mixer_count = tokens // (chips * CORES)
    routed = (chips, ep_count, block_rows, width)
    rows = (chips, tokens_here, width)
    mixed = (chips, mixer_count, width)
    small = (8, 128)
    buffers = [(a.shape, a.dtype) for a in (
        query_rows, key_rows, value_rows, gate_rows, out_weight, expert_gate, expert_up,
        expert_down, shared_gate, shared_up, shared_down,
    )]
    buffers += [
        ((chips, CORES, tokens_here, width + 128), bf16),
        (routed, bf16), ((chips, CORES) + routed[1:], bf16), (routed, bf16), (routed, bf16),
        (routed, bf16), (routed, bf16),
    ]
    buffers += [(rows, bf16)] * 6 + [(mixed, bf16)] * 5
    buffers += [
        (value_rows.shape, bf16), (value_rows.shape, f32), (key_rows.shape, bf16),
        ((blocks, heads, key_width, value_width), f32), ((heads, key_width, value_width), f32),
        ((heads, key_width, value_width), bf16),
        ((ep_count, heads, key_width, value_width), bf16), (small, f32),
        ((ep_count,) + small, f32), ((blocks,) + small, f32), ((blocks * heads, BLOCK), f32),
        ((blocks, 8, BLOCK), f32), ((blocks, BLOCK, 128), f32),
    ]
    one, two, by_ep, by_head = (chips,), (chips, ep_count), (ep_count,), (ep_count, heads)
    counts = [(13,)] + [one] * 5 + [two] * 2 + [one] * 6 + [two] * 2 + [by_head] * 2 + [by_ep] * 2
    counts += [one] * 2 + [(chips, 2)] * 3 + [one] * 3
    return buffers, counts


def whole_step(args, ep_count, chips, capacity):
    (
        query_rows, key_rows, value_rows, gate_rows, log_decay, out_weight, channel_input,
        norm_gain, routes, route_weight, expert_gate, expert_up, expert_down, shared_gate,
        shared_up, shared_down,
    ) = args
    tokens_here, width = channel_input.shape
    tokens, heads = query_rows.shape[0], log_decay.shape[0]
    mixer_count = tokens // (chips * CORES)
    near, far = turn_tables(query_rows.shape[1] // heads, tokens * ep_count)
    buffers, counts = whole_scratch(args, ep_count, chips, capacity)
    vmem = pl.BlockSpec(memory_space=pltpu.VMEM)
    hbm = pl.BlockSpec(memory_space=pl.ANY)
    results = pl.pallas_call(
        functools.partial(whole_kernel, (ep_count, chips, capacity)),
        out_shape=(
            jax.ShapeDtypeStruct((mixer_count, width), jnp.bfloat16),
            jax.ShapeDtypeStruct((tokens_here, width), jnp.bfloat16),
        ),
        in_specs=[vmem] * 7 + [hbm] * 11,
        out_specs=(hbm, hbm),
        scratch_shapes=[pltpu.VMEM(shape, dtype) for shape, dtype in buffers]
        + [pltpu.SemaphoreType.DMA(count) for count in counts],
        compiler_params=pltpu.CompilerParams(
            collective_id=0, has_side_effects=True, vmem_limit_bytes=KERNEL_VMEM
        ),
    )(
        channel_input, norm_gain.reshape(1, width), routes.T, route_weight.T, log_decay,
        jnp.asarray(near), jnp.asarray(far), query_rows, key_rows, value_rows, gate_rows,
        out_weight, expert_gate, expert_up, expert_down, shared_gate, shared_up, shared_down,
    )
    return pl.pallas_call(
        hand_out, out_shape=tuple(jax.ShapeDtypeStruct(r.shape, r.dtype) for r in results),
        in_specs=[vmem] * 2, out_specs=(vmem, vmem),
    )(*results)


def hand_out(mixer_ref, channel_ref, mixer_out_ref, channel_out_ref):
    mixer_out_ref[...] = mixer_ref[...]
    channel_out_ref[...] = channel_ref[...]


def padded_bytes(shape, dtype):
    size = jnp.dtype(dtype).itemsize
    rows = 32 // size
    last = -(-shape[-1] // 128) * 128
    return math.prod(shape[:-2]) * (-(-shape[-2] // rows) * rows) * last * size


def one_kernel_fits(args, ep_count, chips, capacity):
    query_rows, log_decay, experts = args[0], args[4], args[10].shape[0] * ep_count
    heads = log_decay.shape[0]
    buffers, _ = whole_scratch(args, ep_count, chips, capacity)
    need = sum(padded_bytes(shape, dtype) for shape, dtype in buffers)
    return (
        chips > 1
        and capacity % 16 == 0
        and experts <= 128
        and experts * capacity <= 256
        and heads <= 8
        and query_rows.shape[1] // heads == 128
        and args[6].shape[0] % 16 == 0
        and need <= KERNEL_VMEM - (10 << 20)
    )


def local(
    query_rows, key_rows, value_rows, gate_rows, log_decay, out_weight, channel_input, norm_gain,
    routes, route_weight, expert_gate, expert_up, expert_down, shared_gate, shared_up, shared_down,
):
    ep_count, tp_count = lax.axis_size("ep"), lax.axis_size("tp")
    ep_index, tp_index = lax.axis_index("ep"), lax.axis_index("tp")
    chips = tp_count // CORES
    chip, core = tp_index // CORES, tp_index % CORES
    tokens_here, width = channel_input.shape
    topk = routes.shape[1]
    local_experts = expert_gate.shape[0]
    experts_all = ep_count * local_experts
    capacity = tokens_here * topk // experts_all + max(
        2, tokens_here * topk // (3 * experts_all)
    )

    args = (
        query_rows, key_rows, value_rows, gate_rows, log_decay, out_weight, channel_input,
        norm_gain, routes, route_weight, expert_gate, expert_up, expert_down, shared_gate,
        shared_up, shared_down,
    )
    if one_kernel_fits(args, ep_count, chips, capacity):
        return whole_step(args, ep_count, chips, capacity)

    wide = channel_input.astype(jnp.float32)
    normed = (
        wide * lax.rsqrt(jnp.mean(wide * wide, axis=-1, keepdims=True) + epsilon) * norm_gain
    ).astype(jnp.bfloat16)
    flat = routes.reshape(-1)
    onehot = (flat[:, None] == jnp.arange(experts_all, dtype=jnp.int32)[None, :]).astype(
        jnp.float32
    )
    count = tokens_here * topk
    before = (jnp.arange(count)[:, None] > jnp.arange(count)[None, :]).astype(jnp.float32)
    rank = jnp.sum(jnp.dot(before, onehot) * onehot, axis=1)
    notes = jnp.concatenate(
        [routes.astype(jnp.float32), rank.reshape(tokens_here, topk), route_weight], axis=1
    )
    notes = jnp.pad(notes, ((0, 0), (0, 128 - 3 * topk)))
    own_rows = line_gather(normed, chips)
    notes_all = line_gather(notes, chips)
    log_decay, normed, notes = lax.optimization_barrier((log_decay, normed, notes))
    route_all = notes_all[:, :, :topk].astype(jnp.int32)
    rank_all = notes_all[:, :, topk : 2 * topk].astype(jnp.int32)
    weight_all = notes_all[:, :, 2 * topk : 3 * topk]
    place = jnp.arange(chips, dtype=jnp.int32)[:, None, None]
    turn = (route_all // local_experts) ^ ep_index
    slot = ((turn * local_experts + route_all % local_experts) * chips + place) * capacity
    slot = (slot + rank_all).reshape(chips * tokens_here, topk)
    slot_count = experts_all * chips * capacity
    slot_ids = jnp.arange(slot_count, dtype=jnp.int32)
    placing = sum(
        (slot_ids[:, None] == slot[None, :, t]).astype(jnp.bfloat16) for t in range(topk)
    )
    own_flat = own_rows.reshape(chips * tokens_here, width)
    outgoing = jnp.dot(placing, own_flat, preferred_element_type=jnp.float32).astype(jnp.bfloat16)
    outgoing = outgoing.reshape(ep_count, local_experts, chips * capacity, width)
    arrived = [outgoing[0]] + [swap_ep(outgoing[k], k, ep_count) for k in range(1, ep_count)]
    own_twin = swap_cores(own_flat, tp_count)

    gated = retention(query_rows, key_rows, value_rows, gate_rows, log_decay)
    mixer_count = query_rows.shape[0] // tp_count
    gated_parts = gated.reshape(chips, CORES, mixer_count, gated.shape[1])

    def mixer_for(which):
        mine = lax.dynamic_index_in_dim(gated_parts, which, 1, keepdims=False)
        product = jnp.dot(
            mine.reshape(chips * mixer_count, -1), out_weight, preferred_element_type=jnp.float32
        )
        return product.astype(jnp.bfloat16)

    mixer_twin, mixer_mine = mixer_for(1 - core), mixer_for(core)
    mixer_half = summed(mixer_mine, swap_cores(mixer_twin, tp_count))
    arrived, _ = lax.optimization_barrier((arrived, (mixer_twin, mixer_mine)))
    arrived_twin = [swap_cores(block, tp_count) for block in arrived]
    mixer_half = mixer_half.reshape(chips, mixer_count, width)
    mixer_out = line_scatter(
        lambda r: lax.dynamic_index_in_dim(mixer_half, (chip + r) % chips, 0, False), chips
    ).astype(jnp.bfloat16)

    def experts_on(blocks, rows):
        routed = jnp.concatenate(blocks, axis=1)
        gate_part = jnp.einsum("emd,edf->emf", routed, expert_gate, preferred_element_type=jnp.float32)
        up_part = jnp.einsum("emd,edf->emf", routed, expert_up, preferred_element_type=jnp.float32)
        hidden = gated_pair(gate_part, up_part)
        routed_term = jnp.einsum(
            "emf,efd->emd", hidden, expert_down, preferred_element_type=jnp.float32
        ).astype(jnp.bfloat16)
        shared_hidden = gated_pair(
            jnp.dot(rows, shared_gate, preferred_element_type=jnp.float32),
            jnp.dot(rows, shared_up, preferred_element_type=jnp.float32),
        )
        shared_term = jnp.dot(
            shared_hidden, shared_down, preferred_element_type=jnp.float32
        ).astype(jnp.bfloat16)
        return routed_term, shared_term

    routed_twin, shared_twin = experts_on(arrived_twin, own_twin)
    routed_mine, shared_mine = experts_on(arrived, own_flat)
    routed = summed(routed_mine, swap_cores(routed_twin, tp_count))
    shared = summed(shared_mine, swap_cores(shared_twin, tp_count))
    routed = routed.reshape(local_experts, ep_count, chips * capacity, width)
    returned = [routed[:, 0]] + [swap_ep(routed[:, k], k, ep_count) for k in range(1, ep_count)]
    returned = jnp.stack(returned).reshape(slot_count, width)
    flat_weight = weight_all.reshape(chips * tokens_here, topk)
    mixing = sum(
        jnp.where(slot_ids[None, :] == slot[:, t : t + 1], flat_weight[:, t : t + 1], 0.0)
        for t in range(topk)
    )
    coarse = lax.reduce_precision(mixing, 8, 7)
    fine = (mixing - coarse).astype(jnp.bfloat16)
    coarse = coarse.astype(jnp.bfloat16)
    channel = (
        jnp.dot(coarse, returned, preferred_element_type=jnp.float32)
        + jnp.dot(fine, returned, preferred_element_type=jnp.float32)
        + shared.astype(jnp.float32)
    ).astype(jnp.bfloat16)
    channel = channel.reshape(chips, tokens_here, width)
    channel_out = line_scatter(lambda r: channel[(chips - r) % chips], chips).astype(jnp.bfloat16)
    return (mixer_out, channel_out)


def solution(mesh):
    in_specs = (
        P("ep", "tp"),
        P("ep", "tp"),
        P("ep", "tp"),
        P("ep", "tp"),
        P("tp", "ep"),
        P("tp", None),
        P(("ep", "tp"), None),
        P(),
        P(("ep", "tp"), None),
        P(("ep", "tp"), None),
        P("ep", None, "tp"),
        P("ep", None, "tp"),
        P("ep", "tp", None),
        P(None, "tp"),
        P(None, "tp"),
        P("tp", None),
    )
    out_specs = (P(("ep", "tp"), None), P(("ep", "tp"), None))
    return jax.shard_map(local, mesh=mesh, in_specs=in_specs, out_specs=out_specs, check_vma=False)
```
